256 devices in a mesh: ep: 16 (over y, x), tp: 16 (over z, core).
Axes of the slice: x: 4, y: 4, z: 8, core: 2. Of those that a mesh axis runs over, the one named last changes fastest.
Arguments:
- query_preactivation: bfloat16 [32768, 2048], P('ep', 'tp'), may hold values from -6 to 6
- forget_preactivation: bfloat16 [32768, 2048], P('ep', 'tp'), may hold values from -6 to 6
- value_input_rows: bfloat16 [32768, 1024], P('ep', 'tp'), may hold values from -8 to 8
- output_gate_preactivation: bfloat16 [32768, 1024], P('ep', 'tp'), may hold values from -6 to 6
- forget_floor_gap: float32 [2048], P('tp'), may hold values from 0 to 0.2, as said below
- extra_log_forget: float32 [32768, 16], P('ep', 'tp'), may hold values from -2 to 0
- head_output_gain: float32 [1024], P('tp'), may hold values from 0.1 to 1.9
- mixer_output_weight: bfloat16 [1024, 2048], P(None, 'tp'), may hold values from -0.1875 to 0.1875
- second_batch_tokens: bfloat16 [8192, 2048], P('ep'), may hold values from -6 to 6
- feedforward_norm_gain: float32 [2048], replicated, may hold values from 0.1 to 1.9
- chosen_expert_index: int32 [8192, 2], P('ep'), may hold values from 0 to 15, all different within a row; in each aligned block of 32 rows (0 to 31, 32 to 63, ...) at most 5 rows name the same one
- chosen_expert_weight: float32 [8192, 2], P('ep'), may hold values from 0.1 to 1
- expert_gate_weight: bfloat16 [16, 2048, 7168], P('ep', None, 'tp'), may hold values from -0.125 to 0.125
- expert_up_weight: bfloat16 [16, 2048, 7168], P('ep', None, 'tp'), may hold values from -0.125 to 0.125
- expert_down_weight: bfloat16 [16, 7168, 2048], P('ep', 'tp'), may hold values from -0.0625 to 0.0625
Outputs:
- mixer_output_first: bfloat16 [32768, 2048], P('ep', 'tp')
- moe_out: bfloat16 [8192, 2048], P(('ep', 'tp'))
The draws below stay inside these ranges and needn't reach their ends.
Inputs may be any that keep to these rules, and one draw needn't show every extreme that they name: `chosen_expert_index`: each row names 2 different experts. In each aligned block of 32 rows (the rows of one device's share) no expert is named by more than 5 rows, and in every draw some expert is named by exactly 5 rows of some block. `forget_floor_gap`: every entry is positive.
All inputs are finite; a program needn't handle non-finite values.
Results may differ from the reference program's by a relative error of at most 0.019.
Values may be sent and summed in bfloat16 or wider, within the bound.
A program may use at most 128 MiB of HBM per device.

```python
import math
import jax
import jax.numpy as jnp
import numpy as np
from jax import lax

D = 2048
RECURRENT_HEADS = 16
KEY_DIM = 128
VAL_DIM = 64
KW = 2048
VW = 1024
BLOCK_POSITIONS = 64
SEG_A = 2048
TOKENS_A = 32768
TOKENS_B = 8192
SUB_B = 32
EXPERTS = 16
FFE = 7168
FFE_DEV = 448
TOPK = 2
CAP = 5
N_TP = 16


def draw_value_input_rows(key, part):
    noise_key, offset_key = jax.random.split(key)
    noise_part = jnp.clip(jax.random.normal(noise_key, (TOKENS_A, VW), jnp.float32), -6.0, 6.0)
    offsets = jax.random.uniform(offset_key, (1, VW), jnp.float32, -1.0, 1.0)
    return (noise_part + offsets).astype(jnp.bfloat16)


def draw_forget_floor_gap(key, part):
    choose_key, slow_key, fast_key = jax.random.split(key, 3)
    slow_share = 0.5
    chosen = jax.random.uniform(choose_key, (KW,), jnp.float32) < slow_share
    slow_rate = jnp.exp(jax.random.uniform(slow_key, (KW,), jnp.float32, jnp.log(0.05 / TOKENS_A), jnp.log(1.0 / TOKENS_A)))
    fast_rate = jnp.exp(jax.random.uniform(fast_key, (KW,), jnp.float32, jnp.log(0.06), jnp.log(0.2)))
    return jnp.where(chosen, slow_rate, fast_rate)


def draw_extra_log_forget(key, part):
    rate_key, place_key, depth_key = jax.random.split(key, 3)
    segments = TOKENS_A // SEG_A
    rates = jnp.exp(jax.random.uniform(rate_key, (segments, 1, RECURRENT_HEADS), jnp.float32, jnp.log(0.1 / TOKENS_A), jnp.log(0.4 / TOKENS_A)))
    base_log = -jnp.broadcast_to(rates, (segments, SEG_A, RECURRENT_HEADS)).reshape(TOKENS_A, RECURRENT_HEADS)
    places = jax.random.randint(place_key, (2, RECURRENT_HEADS), 0, TOKENS_A)
    depths = jax.random.uniform(depth_key, (2, RECURRENT_HEADS), jnp.float32, jnp.log(0.5), jnp.log(0.8))
    columns = jnp.broadcast_to(jnp.arange(RECURRENT_HEADS, dtype=jnp.int32)[None, :], (2, RECURRENT_HEADS))
    return base_log.at[places, columns].add(depths)


def block_scale(own_key, shape, shards, least, high):
    level, own = 1.0, jax.random.fold_in(own_key, 6)
    for axis_at, shards_of in shards:
        heights = jnp.exp(jax.random.uniform(jax.random.fold_in(own, axis_at), (shards_of,), jnp.float32, least / len(shards), high / len(shards)))
        level = level * jnp.repeat(heights, shape[axis_at] // shards_of).reshape([-1 if axis == axis_at else 1 for axis in range(len(shape))])
    return level


def assign_block(own_key, own, number, rows, count, top, limit, lean):
    ranking = jax.random.permutation(own_key, count)
    crowded, usual = portions_of(count, rows * top, limit, lean, True), portions_of(count, rows * top, limit, lean, False)
    places = jnp.arange(count)

    def named(lengths, turn):
        used = int((lengths > 0).sum())
        fixed = max(1, used // 4)
        shifted = fixed + (places - fixed + turn * (used - fixed)) % max(1, count - fixed)
        return jnp.zeros((count,), jnp.int32).at[ranking[jnp.where(places < fixed, places, shifted)]].set(jnp.asarray(lengths, jnp.int32))

    lengths = jnp.where(number % 4 == 0, named(crowded, number // 4), named(usual, number - number // 4 - 1))
    mixed = jax.random.permutation(jax.random.fold_in(own, 3), count)
    giver, receiver = mixed[0:count // 2 * 2:2], mixed[1:count // 2 * 2:2]
    room = jnp.minimum(lengths[giver] - 1, limit - lengths[receiver]) // 2
    room = jnp.where((giver == ranking[0]) | (receiver == ranking[0]) | (lengths[receiver] == 0), 0, jnp.maximum(room, 0))
    shifted = jax.random.randint(jax.random.fold_in(own, 4), (count // 2,), 0, 1 << 20) % (room + 1)
    lengths = lengths.at[giver].add(-shifted).at[receiver].add(shifted)
    labels = jnp.searchsorted(jnp.cumsum(lengths), jnp.arange(rows * top), side="right").astype(jnp.int32)
    listing = labels.reshape(top, rows).T
    listing = listing[jax.random.permutation(jax.random.fold_in(own, 1), rows)]
    turn = jax.random.randint(jax.random.fold_in(own, 2), (rows, 1), 0, top)
    return jnp.take_along_axis(listing, (jnp.arange(top)[None, :] + turn) % top, axis=1)


def portions_of(amount, total, reach, skew, full):
    portions = [(1 << 20) // math.isqrt(grade ** skew) + 1 for grade in range(1, amount + 1)]
    largest = reach if full else min(reach, max(-(-total // amount), total * portions[0] // sum(portions)))
    least = 1 if total - largest >= amount - 1 else 0
    counts, spare = [largest] + [least] * (amount - 1), total - largest - least * (amount - 1)
    while spare > 0:
        candidates = [i for i in range(1, amount) if counts[i] < largest] or [i for i in range(1, amount) if counts[i] < reach]
        pool, left = sum([portions[i] for i in candidates]), spare
        for i in candidates:
            more = min(reach - counts[i], max(1, left * portions[i] // pool), spare)
            counts[i] = counts[i] + more
            spare = spare - more
    return np.array(counts)


def scatter_about(own_key, dims, deviation, bound, cuts=(), kind=jnp.bfloat16):
    array = deviation * jax.random.normal(own_key, dims, jnp.float32)
    if cuts:
        array = array * block_scale(own_key, dims, cuts, -0.22, 0.18)
    return jnp.clip(array, -bound, bound).astype(kind)


def setup_inputs(seed: int = 0) -> dict:
    key_of = jax.random.split(jax.random.key(seed), 16)
    query_preactivation = scatter_about(key_of[0], (TOKENS_A, KW), 1.0, 6.0, ((0, 16), (1, 16)))
    forget_preactivation = scatter_about(key_of[1], (TOKENS_A, KW), 1.0, 6.0, ((0, 16), (1, 16)))
    value_input_rows = draw_value_input_rows(jax.random.fold_in(key_of[15], 71), 0)
    output_gate_preactivation = scatter_about(key_of[3], (TOKENS_A, VW), 1.0, 6.0, ((0, 16), (1, 16)))
    forget_floor_gap = draw_forget_floor_gap(jax.random.fold_in(key_of[15], 71), 0)
    extra_log_forget = draw_extra_log_forget(jax.random.fold_in(key_of[15], 71), 0)
    head_output_gain = jnp.clip(1.0 + 0.18 * jax.random.normal(key_of[6], (VW,), jnp.float32), 0.1, 1.9)
    mixer_output_weight = scatter_about(key_of[7], (VW, D), VW ** -0.5, 0.1875, ((1, 16),))
    second_batch_tokens = scatter_about(key_of[8], (TOKENS_B, D), 1.0, 6.0, ((0, 16),))
    feedforward_norm_gain = jnp.clip(1.0 + 0.18 * jax.random.normal(key_of[9], (D,), jnp.float32), 0.1, 1.9)
    chosen_expert_index_keys = jax.random.split(jax.random.fold_in(key_of[10], 1), TOKENS_B // SUB_B)
    chosen_expert_index_turns = jax.random.permutation(jax.random.fold_in(key_of[10], 3), TOKENS_B // SUB_B)
    chosen_expert_index = jax.vmap(lambda own, number: assign_block(jax.random.fold_in(key_of[10], 2), own, number, SUB_B, EXPERTS, TOPK, CAP, 1))(chosen_expert_index_keys, chosen_expert_index_turns).reshape((TOKENS_B, TOPK))
    chosen_expert_weight = jnp.clip(0.1 + 0.9 * jax.random.uniform(key_of[11], (TOKENS_B, TOPK), jnp.float32) ** block_scale(key_of[11], (TOKENS_B, TOPK), ((0, 16),), -0.2, 0.2), 0.1, 1.0)
    expert_gate_weight = scatter_about(key_of[12], (EXPERTS, D, FFE), D ** -0.5, 0.125, ((0, 16), (2, 16)))
    expert_up_weight = scatter_about(key_of[13], (EXPERTS, D, FFE), D ** -0.5, 0.125, ((0, 16), (2, 16)))
    expert_down_weight = scatter_about(key_of[14], (EXPERTS, FFE, D), FFE ** -0.5, 0.0625, ((0, 16), (1, 16)))
    return {"query_preactivation": query_preactivation, "forget_preactivation": forget_preactivation, "value_input_rows": value_input_rows, "output_gate_preactivation": output_gate_preactivation, "forget_floor_gap": forget_floor_gap, "extra_log_forget": extra_log_forget, "head_output_gain": head_output_gain, "mixer_output_weight": mixer_output_weight, "second_batch_tokens": second_batch_tokens, "feedforward_norm_gain": feedforward_norm_gain, "chosen_expert_index": chosen_expert_index, "chosen_expert_weight": chosen_expert_weight, "expert_gate_weight": expert_gate_weight, "expert_up_weight": expert_up_weight, "expert_down_weight": expert_down_weight}


highest_accuracy = lax.Precision.HIGHEST
epsilon = 1e-06

def slot_positions(blocks):
    flattened = blocks.reshape(blocks.shape[0], -1)
    onehot = (flattened[..., None] == jnp.arange(EXPERTS, dtype=jnp.int32)).astype(jnp.int32)
    earlier = jnp.cumsum(onehot, axis=1) - onehot
    return lax.optimization_barrier(jnp.sum(earlier * onehot, axis=-1)).reshape(blocks.shape)

def mixer_portion(query_preactivation, forget_preactivation, value_input_rows, output_gate_preactivation, forget_floor_gap, extra_log_forget, head_output_gain, mixer_output_weight):
    length = query_preactivation.shape[0]
    block_count = length // BLOCK_POSITIONS
    shape_key = (block_count, BLOCK_POSITIONS, RECURRENT_HEADS, KEY_DIM)
    queries = jax.nn.silu(query_preactivation.astype(jnp.float32)).reshape(shape_key)
    key_decay_rates = forget_floor_gap.reshape(RECURRENT_HEADS, KEY_DIM) * jax.nn.sigmoid(-forget_preactivation.astype(jnp.float32)).reshape(shape_key)
    forget_log_factor = jnp.log(1.0 - key_decay_rates) + extra_log_forget.reshape(block_count, BLOCK_POSITIONS, RECURRENT_HEADS)[..., None]
    values = value_input_rows.astype(jnp.float32).reshape(block_count, BLOCK_POSITIONS, RECURRENT_HEADS, VAL_DIM)
    causal_mask = jnp.arange(BLOCK_POSITIONS)[:, None] >= jnp.arange(BLOCK_POSITIONS)[None, :]

    def advance(recurrent_state_matrix, inputs):
        query_block_rows, block_key, value_block_rows, block_log = inputs
        cumulative_log = jnp.cumsum(block_log, axis=0)
        block_final_row = cumulative_log[-1]
        query_scaled = query_block_rows * jnp.exp(cumulative_log - block_final_row)
        scaled_key_rows = block_key * jnp.exp(block_final_row - cumulative_log)
        scores = jnp.einsum('thk,shk->hts', query_scaled, scaled_key_rows, precision=highest_accuracy)
        scores = jnp.where(causal_mask, scores, 0.0)
        within = jnp.einsum('hts,shv->thv', scores, value_block_rows, precision=highest_accuracy)
        across_blocks = jnp.einsum('pjy,jyr->pjr', query_block_rows * jnp.exp(cumulative_log), recurrent_state_matrix, precision=highest_accuracy)
        recurrent_state_matrix = jnp.exp(block_final_row)[..., None] * recurrent_state_matrix + jnp.einsum('jnz,jne->nze', scaled_key_rows, value_block_rows, precision=highest_accuracy)
        return (recurrent_state_matrix, within + across_blocks)
    initial = jnp.zeros((RECURRENT_HEADS, KEY_DIM, VAL_DIM), jnp.float32)
    final_state, outputs = lax.scan(advance, initial, (queries, key_decay_rates, values, forget_log_factor))
    recurrent = outputs.reshape(length, RECURRENT_HEADS, VAL_DIM)
    factor = lax.rsqrt(lax.optimization_barrier(jnp.mean(recurrent * recurrent, axis=-1, keepdims=True)) + epsilon)
    normed = (recurrent * factor * head_output_gain.reshape(RECURRENT_HEADS, VAL_DIM)).reshape(length, RECURRENT_HEADS * VAL_DIM)
    mixed = (normed * jax.nn.silu(output_gate_preactivation.astype(jnp.float32))).astype(jnp.bfloat16)
    return jnp.dot(mixed, mixer_output_weight, preferred_element_type=jnp.float32).astype(jnp.bfloat16)

def expert_part(second_batch_tokens, feedforward_norm_gain, chosen_expert_index, chosen_expert_weight, expert_gate_weight, expert_up_weight, expert_down_weight):
    total_rows = second_batch_tokens.shape[0]
    width = second_batch_tokens.shape[1]
    tokens_float = second_batch_tokens.astype(jnp.float32)
    factor = lax.rsqrt(lax.optimization_barrier(jnp.mean(tokens_float * tokens_float, axis=-1, keepdims=True)) + epsilon)
    normed = (tokens_float * factor * feedforward_norm_gain).astype(jnp.bfloat16)
    nsub = total_rows // SUB_B
    blocks = chosen_expert_index.reshape(nsub, SUB_B, TOPK)
    slot_ids = slot_positions(blocks)
    sub_index = jnp.arange(nsub, dtype=jnp.int32)[:, None, None]
    flat_slot = (blocks * nsub + sub_index) * CAP + slot_ids
    token_ids = jnp.broadcast_to(jnp.arange(total_rows, dtype=jnp.int32).reshape(nsub, SUB_B, 1), blocks.shape)
    lookup = jnp.full((EXPERTS * nsub * CAP,), -1, jnp.int32).at[flat_slot.reshape(-1)].set(token_ids.reshape(-1))
    lookup = lookup.reshape(EXPERTS, nsub * CAP)

    def one_expert(inputs):
        row_index, gate_weight, up_weight, down_weight = inputs
        picked = normed[jnp.maximum(row_index, 0)]
        routed = jnp.where((row_index >= 0)[:, None], picked, jnp.zeros((), jnp.bfloat16))
        gate_part = jnp.dot(routed, gate_weight, preferred_element_type=jnp.float32)
        up_part = jnp.dot(routed, up_weight, preferred_element_type=jnp.float32)
        hidden = (jax.nn.silu(gate_part) * up_part).astype(jnp.bfloat16)
        hidden_groups = jnp.transpose(hidden.reshape(-1, N_TP, FFE_DEV), (1, 0, 2))
        down_groups = down_weight.reshape(N_TP, FFE_DEV, width)

        def add_group(running, pair):
            product = jnp.dot(pair[0], pair[1], preferred_element_type=jnp.float32)
            return (running + lax.optimization_barrier(product.astype(jnp.bfloat16)).astype(jnp.float32), None)
        running, unused = lax.scan(add_group, jnp.zeros((hidden.shape[0], width), jnp.float32), (hidden_groups, down_groups))
        return running.astype(jnp.bfloat16)
    outputs = lax.map(one_expert, (lookup, expert_gate_weight, expert_up_weight, expert_down_weight))
    flat_outputs = outputs.reshape(-1, width)
    flat_index = flat_slot.reshape(total_rows, TOPK)
    combined = jnp.zeros((total_rows, width), jnp.float32)
    for ranked in range(TOPK):
        combined = combined + flat_outputs[flat_index[:, ranked]].astype(jnp.float32) * chosen_expert_weight[:, ranked:ranked + 1]
    return combined.astype(jnp.bfloat16)

def reference(query_preactivation, forget_preactivation, value_input_rows, output_gate_preactivation, forget_floor_gap, extra_log_forget, head_output_gain, mixer_output_weight, second_batch_tokens, feedforward_norm_gain, chosen_expert_index, chosen_expert_weight, expert_gate_weight, expert_up_weight, expert_down_weight):
    mixer_output_first = mixer_portion(query_preactivation, forget_preactivation, value_input_rows, output_gate_preactivation, forget_floor_gap, extra_log_forget, head_output_gain, mixer_output_weight)
    moe_out = expert_part(second_batch_tokens, feedforward_norm_gain, chosen_expert_index, chosen_expert_weight, expert_gate_weight, expert_up_weight, expert_down_weight)
    return (mixer_output_first, moe_out)
```

```python
import functools

import jax
import jax.numpy as jnp
from jax import lax
from jax.experimental import pallas as pl
from jax.experimental.pallas import tpu as pltpu
from jax.sharding import PartitionSpec as P

KEY_DIM = 128
VAL_DIM = 64
BLOCK = 64
PAIR = 128
TOPK = 2
EPS = 1e-06
MESH = pl.DeviceIdType.MESH
F32 = jnp.float32
BF16 = jnp.bfloat16
NT = (((1,), (1,)), ((), ()))


def offsets(experts):
    if experts == 16:
        return [
            (0, 0), (0, 1), (3, 0), (0, 3),
            (1, 0), (1, 1), (3, 3), (1, 3),
            (3, 1), (0, 2), (2, 0), (1, 2),
            (2, 3), (3, 2), (2, 1), (2, 2),
        ]
    return [(0, k) for k in range(experts)]


def moved(me, step, experts, back=False):
    dy, dx = step
    if experts != 16:
        return lax.rem(me + (experts - dx if back else dx), experts)
    y, x = me // 4, lax.rem(me, 4)
    if back:
        dy, dx = (4 - dy) % 4, (4 - dx) % 4
    return lax.rem(y + dy, 4) * 4 + lax.rem(x + dx, 4)


def kernel(
    cfg,
    q_hbm, f_hbm, v_hbm, o_hbm, gap_ref, extra_ref, hgain_ref, wo_hbm,
    x_hbm, fgain_ref, idx_ref, wt_ref, wg_hbm, wu_hbm, wd_hbm,
    out_hbm, moe_ref,
    q_s, f_s, v_s, o_s, wo_s, x_s, wg_s, wu_s, wd_s,
    tri_s, dec_s, pre_s, yw_s, qe_s, cs_s, cr_s,
    n_s, slot_s, g_s, s_s, r_s, hid_s, pp_s, qb_s, rb_s,
    m_s, out_s, fs_s, rr_s, gh_s, gl_s, co_s, fo_s,
    lsem, osem, asend, arecv, fsend, frecv, csend, crecv,
    msend, mrecv, dsend, drecv, psend, precv, bsend, brecv, rsend, rrecv, zsend, zrecv,
):
    E, TP, TOK, SUB, CAP = cfg["E"], cfg["TP"], cfg["TOK"], cfg["SUB"], cfg["CAP"]
    Z = TP // 2
    KR = TP * CAP
    KG = max(1, E // 4)
    NG = E // KG
    GR = KG * KR
    D = x_hbm.shape[1]
    H = D // 2
    NTOK = x_hbm.shape[0]
    offs = offsets(E)
    me = lax.axis_index("ep")
    t = lax.axis_index("tp")
    z, c = t // 2, lax.rem(t, 2)
    pc = 1 - c

    def remote(src, dst, ss, rs, e, tt):
        return pltpu.make_async_remote_copy(
            src_ref=src, dst_ref=dst, send_sem=ss, recv_sem=rs, device_id=(e, tt), device_id_type=MESH
        )

    loads = [
        (x_hbm.at[:, 0:H], x_s.at[0]), (x_hbm.at[:, H:D], x_s.at[1]),
        (f_hbm, f_s), (q_hbm, q_s), (v_hbm, v_s), (o_hbm, o_s),
        (wg_hbm, wg_s), (wu_hbm, wu_s), (wd_hbm, wd_s), (wo_hbm, wo_s),
    ]
    loads = [pltpu.make_async_copy(a, b, lsem.at[i]) for i, (a, b) in enumerate(loads)]
    for load in loads:
        load.start()
    barrier = pltpu.get_barrier_semaphore()
    for k in range(1, E):
        pl.semaphore_signal(barrier, inc=1, device_id=(moved(me, offs[k], E), t), device_id_type=MESH)
    for j in range(1, TP):
        pl.semaphore_signal(barrier, inc=1, device_id=(me, lax.rem(t + j, TP)), device_id_type=MESH)

    i0, i1 = idx_ref[0:1, :], idx_ref[1:2, :]
    row_e = lax.broadcasted_iota(jnp.int32, (E, NTOK), 0)
    expert_of = jnp.zeros((E, NTOK), jnp.int32)
    for k in range(E):
        expert_of = jnp.where(row_e == k, moved(me, offs[k], E), expert_of)
    first, second = expert_of == i0, expert_of == i1
    chosen = jnp.where(first | second, 1.0, 0.0)
    ra = lax.broadcasted_iota(jnp.int32, (NTOK, NTOK), 0)
    rb = lax.broadcasted_iota(jnp.int32, (NTOK, NTOK), 1)
    before = jnp.where((ra // SUB == rb // SUB) & (ra < rb), 1.0, 0.0).astype(BF16)
    place = jnp.dot(chosen.astype(BF16), before, preferred_element_type=F32)
    block_of = (lax.broadcasted_iota(jnp.int32, (E, NTOK), 1) // SUB).astype(F32)
    slot_s[...] = jnp.where(chosen > 0, CAP * block_of + place, -1.0)
    weight = jnp.where(first, wt_ref[0:1, :], 0.0) + jnp.where(second, wt_ref[1:2, :], 0.0)
    weight_hi = weight.astype(BF16)
    weight_lo = (weight - weight_hi.astype(F32)).astype(BF16)

    loads[0].wait()
    loads[1].wait()
    gain_half = fgain_ref[:, pl.ds(pl.multiple_of(c * H, 128), H)]

    def norm_rows(i, carry):
        rows = pl.ds(pl.multiple_of(i * 64, 64), 64)
        a, b = x_s[0, rows, :].astype(F32), x_s[1, rows, :].astype(F32)
        total = jnp.sum(a * a + b * b, axis=-1, keepdims=True)
        factor = lax.rsqrt(total / D + EPS)
        n_s[rows, :] = (x_s[c, rows, :].astype(F32) * factor * gain_half).astype(BF16)
        return carry

    lax.fori_loop(0, NTOK // 64, norm_rows, 0)

    place_row = lax.broadcasted_iota(jnp.int32, (KR, NTOK), 0).astype(F32)

    def fill_group(g):
        for k in range(g * KG, (g + 1) * KG):
            rows = slice(k * KR, (k + 1) * KR)
            g_s[rows, :] = jnp.where(place_row == slot_s[k : k + 1, :], 1.0, 0.0).astype(BF16)
        rows = slice(g * GR, (g + 1) * GR)
        pick = g_s[rows, :]
        for n in range(0, H, 256):
            s_s[rows, n : n + 256] = jnp.dot(
                pick, n_s[:, n : n + 256], preferred_element_type=F32
            ).astype(BF16)

    def dispatch(k):
        rows = slice(k * KR, (k + 1) * KR)
        return remote(
            s_s.at[rows, :], r_s.at[c, rows, :], asend.at[k], arecv.at[k], moved(me, offs[k], E), t
        )

    def forward(k):
        rows = slice(k * KR, (k + 1) * KR)
        return remote(
            r_s.at[c, rows, :], r_s.at[c, rows, :], fsend.at[k], frecv.at[k], me, z * 2 + pc
        )

    fill_group(0)
    r_s[c, 0:KR, :] = s_s[0:KR, :]
    pl.semaphore_wait(barrier, E - 1 + TP - 1)
    for k in range(1, KG):
        dispatch(k).start()

    ta = lax.broadcasted_iota(jnp.int32, (PAIR, PAIR), 0)
    tb = lax.broadcasted_iota(jnp.int32, (PAIR, PAIR), 1)
    tri = (ta // BLOCK == tb // BLOCK) & (ta >= tb)
    tri_s[...] = jnp.where(tri, 1.0, 0.0)
    gap = gap_ref[...]
    for load in loads[2:6]:
        load.wait()
    U1 = min(4, TOK // PAIR)

    def local_pairs(i, carry):
        state, decay = carry
        trif = tri_s[...]
        trib = trif.astype(BF16)
        in_first = lax.broadcasted_iota(jnp.int32, (PAIR, PAIR), 0) < BLOCK
        left = lax.broadcasted_iota(jnp.int32, (BLOCK, PAIR), 1) < BLOCK
        later = lax.broadcasted_iota(jnp.int32, (PAIR, PAIR), 1)
        earlier = lax.broadcasted_iota(jnp.int32, (PAIR, PAIR), 0)
        maskt = (later // BLOCK == earlier // BLOCK) & (earlier <= later)
        at = [pl.multiple_of((i * U1 + u) * PAIR, PAIR) for u in range(U1)]
        keys, cums = [], []
        for u in range(U1):
            gate = f_s[pl.ds(at[u], PAIR), :].astype(F32)
            key = gap * (1.0 / (1.0 + jnp.exp(gate)))
            logf = jnp.log(1.0 - key)
            hi = logf.astype(BF16)
            lo = (logf - hi.astype(F32)).astype(BF16)
            cum = jnp.dot(trib, hi, preferred_element_type=F32) + jnp.dot(
                trib, lo, preferred_element_type=F32
            )
            extra = jnp.sum(trif * extra_ref[:, pl.ds(at[u], PAIR)], axis=-1, keepdims=True)
            keys.append(key)
            cums.append(cum + extra)
        work = []
        for u in range(U1):
            key, cum = keys[u], cums[u]
            mid0, mid1 = cum[31:32, :], cum[95:96, :]
            end0, end1 = cum[63:64, :], cum[127:128, :]
            away = cum - jnp.where(in_first, mid0, mid1)
            query = q_s[pl.ds(at[u], PAIR), :].astype(F32)
            query = query * (1.0 / (1.0 + jnp.exp(-query)))
            qs = query * jnp.exp(away)
            ks = key * jnp.exp(-away)
            qe = qs * jnp.where(in_first, jnp.exp(mid0), jnp.exp(mid1))
            ke = ks * jnp.where(in_first, jnp.exp(end0 - mid0), jnp.exp(end1 - mid1))
            qe_s[pl.ds(at[u], PAIR), :] = qe.astype(BF16)
            work.append((qs.astype(BF16), ks.astype(BF16), ke.astype(BF16), jnp.exp(end0), jnp.exp(end1)))
        scores = [lax.dot_general(w[1], w[0], NT, preferred_element_type=F32) for w in work]
        updates = []
        for u in range(U1):
            vt = v_s[:, pl.ds(at[u], PAIR)]
            both = jnp.where(maskt, scores[u], 0.0).astype(BF16)
            yw_s[:, pl.ds(at[u], PAIR)] = jnp.dot(vt, both, preferred_element_type=F32)
            zero = jnp.zeros_like(vt)
            split = jnp.concatenate([jnp.where(left, vt, zero), jnp.where(left, zero, vt)], axis=0)
            updates.append(jnp.dot(split, work[u][2], preferred_element_type=F32))
        for u in range(U1):
            d0, d1 = work[u][3], work[u][4]
            middle = d0 * state + updates[u][0:BLOCK, :]
            pre_s[pl.ds(at[u], BLOCK), :] = state
            pre_s[pl.ds(pl.multiple_of(at[u] + BLOCK, BLOCK), BLOCK), :] = middle
            half = decay * d0
            dec_s[pl.ds(pl.multiple_of((i * U1 + u) * 8, 8), 8), :] = jnp.concatenate(
                [decay, half, jnp.zeros((6, KEY_DIM), F32)], axis=0
            )
            state = d1 * middle + updates[u][BLOCK:PAIR, :]
            decay = half * d1
        return state, decay

    state, decay = lax.fori_loop(
        0, TOK // (PAIR * U1), local_pairs,
        (jnp.zeros((VAL_DIM, KEY_DIM), F32), jnp.ones((1, KEY_DIM), F32)),
    )
    decay_hi = decay.astype(BF16).astype(F32)
    row16 = lax.broadcasted_iota(jnp.int32, (16, KEY_DIM), 0)
    tail = jnp.where(row16 == 0, decay_hi, jnp.where(row16 == 1, decay - decay_hi, 0.0))
    cs_s[0:VAL_DIM, :] = state.astype(BF16)
    cs_s[VAL_DIM : VAL_DIM + 16, :] = tail.astype(BF16)
    cr_s[me] = jnp.zeros((VAL_DIM + 16, KEY_DIM), BF16)

    def hand_on(k):
        return remote(cs_s, cr_s.at[me], csend.at[k], crecv.at[me], moved(me, offs[k], E), t)

    def handed(k):
        source = moved(me, offs[k], E, back=True)
        return remote(cs_s, cr_s.at[source], csend.at[k], crecv.at[source], source, t)

    for k in range(1, E):
        hand_on(k).start()
    for g in range(1, NG):
        fill_group(g)
        for k in range(g * KG, (g + 1) * KG):
            dispatch(k).start()

    for k in range(1, E):
        handed(k).wait_recv()
    start = jnp.zeros((VAL_DIM, KEY_DIM), F32)
    for j in range(E - 1):
        ends = cr_s[j, VAL_DIM : VAL_DIM + 16, :].astype(F32)
        after = (ends[0:1, :] + ends[1:2, :]) * start + cr_s[j, 0:VAL_DIM, :].astype(F32)
        start = jnp.where(j < me, after, start)
    ga = lax.broadcasted_iota(jnp.int32, (VAL_DIM, VAL_DIM), 0)
    gb = lax.broadcasted_iota(jnp.int32, (VAL_DIM, VAL_DIM), 1)
    head_gain = jnp.sum(jnp.where(ga == gb, hgain_ref[...], 0.0), axis=-1, keepdims=True)
    own_rows = pl.multiple_of(t * VAL_DIM, VAL_DIM)

    def finish_pairs(i, carry):
        left = lax.broadcasted_iota(jnp.int32, (BLOCK, PAIR), 1) < BLOCK
        at = [pl.multiple_of((i * U1 + u) * PAIR, PAIR) for u in range(U1)]
        across = []
        for u in range(U1):
            d = dec_s[pl.ds(pl.multiple_of((i * U1 + u) * 8, 8), 8), :]
            s0 = pre_s[pl.ds(at[u], BLOCK), :] + d[0:1, :] * start
            s1 = pre_s[pl.ds(pl.multiple_of(at[u] + BLOCK, BLOCK), BLOCK), :] + d[1:2, :] * start
            states = jnp.concatenate([s0, s1], axis=0).astype(BF16)
            across.append(
                lax.dot_general(states, qe_s[pl.ds(at[u], PAIR), :], NT, preferred_element_type=F32)
            )
        for u in range(U1):
            cols = pl.ds(at[u], PAIR)
            y = yw_s[:, cols] + jnp.where(left, across[u][0:BLOCK, :], across[u][BLOCK:PAIR, :])
            factor = lax.rsqrt(jnp.mean(y * y, axis=0, keepdims=True) + EPS)
            gate = o_s[:, cols].astype(F32)
            gate = gate * (1.0 / (1.0 + jnp.exp(-gate)))
            m_s[pl.ds(own_rows, VAL_DIM), cols] = (y * factor * head_gain * gate).astype(BF16)
        return carry

    lax.fori_loop(0, TOK // (PAIR * U1), finish_pairs, 0)

    VH = VAL_DIM // 2
    reach = {(1, 0): Z // 2, (1, 1): Z - 1 - Z // 2, (-1, 0): Z - 1 - Z // 2, (-1, 1): Z // 2}

    def head_at(zz, core):
        return pl.multiple_of((lax.rem(zz + 2 * Z, Z) * 2 + core) * VAL_DIM, VAL_DIM)

    def ring(way, half, hop):
        rows = pl.ds(pl.multiple_of(head_at(z - way * (hop - 1), c) + half * VH, VH), VH)
        w = 0 if way == 1 else 1
        return remote(
            m_s.at[rows, :], m_s.at[rows, :], msend.at[w, half, hop - 1], mrecv.at[w, half, hop - 1],
            me, lax.rem(z + way + Z, Z) * 2 + c,
        )

    def ringed(way, half, hop):
        rows = pl.ds(pl.multiple_of(head_at(z - way * hop, c) + half * VH, VH), VH)
        w = 0 if way == 1 else 1
        return remote(
            m_s.at[rows, :], m_s.at[rows, :], msend.at[w, half, hop - 1], mrecv.at[w, half, hop - 1],
            me, lax.rem(z + way + Z, Z) * 2 + c,
        )

    def share(r, core):
        rows = pl.ds(head_at(z - r, core), VAL_DIM)
        return remote(m_s.at[rows, :], m_s.at[rows, :], dsend.at[r], drecv.at[r], me, z * 2 + pc)

    lanes = [(1, 0), (-1, 1), (1, 1), (-1, 0)]

    def relay(hop):
        for way, half in lanes:
            if hop <= reach[way, half]:
                ringed(way, half, hop).wait_recv()
                if hop + 1 <= reach[way, half]:
                    ring(way, half, hop + 1).start()
        if hop == Z - hop:
            share(hop, c).start()
        elif hop < Z - hop:
            share(hop, c).start()
            share(Z - hop, c).start()

    for way, half in lanes:
        if reach[way, half] >= 1:
            ring(way, half, 1).start()
    share(0, c).start()

    def forward_group(g):
        for k in range(g * KG, (g + 1) * KG):
            if k:
                dispatch(k).wait_recv()
            forward(k).start()

    def ffn(g):
        rows = slice(g * GR, (g + 1) * GR)
        for k in range(g * KG, (g + 1) * KG):
            back = slice(k * KR, (k + 1) * KR)
            remote(
                r_s.at[c, back, :], r_s.at[pc, back, :], fsend.at[k], frecv.at[k], me, z * 2 + pc
            ).wait_recv()
        a, b = r_s[0, rows, :], r_s[1, rows, :]
        gate = lax.dot_general(a, wg_s[:, 0:H], NT, preferred_element_type=F32) + lax.dot_general(
            b, wg_s[:, H:D], NT, preferred_element_type=F32
        )
        up = lax.dot_general(a, wu_s[:, 0:H], NT, preferred_element_type=F32) + lax.dot_general(
            b, wu_s[:, H:D], NT, preferred_element_type=F32
        )
        hid_s[...] = (gate * (1.0 / (1.0 + jnp.exp(-gate))) * up).astype(BF16)
        hid = hid_s[...]
        for zz in range(Z):
            y = jnp.dot(hid, wd_s[:, zz * 256 : zz * 256 + 256], preferred_element_type=F32).astype(BF16)
            pp_s[0, zz, rows, :] = y[:, 0:128]
            pp_s[1, zz, rows, :] = y[:, 128:256]
        swap(g).start()

    def swap(g):
        rows = slice(g * GR, (g + 1) * GR)
        return remote(
            pp_s.at[pc, :, rows, :], qb_s.at[:, rows, :], psend.at[g], precv.at[g], me, z * 2 + pc
        )

    def way_of(g):
        return 1 if g % 2 == 0 else -1

    def pass_on(g, s):
        way = way_of(g)
        rows = slice(g * GR, (g + 1) * GR)
        part = lax.rem(z - way * (1 + s) + 2 * Z, Z)
        return remote(
            pp_s.at[c, part, rows, :], rb_s.at[s, rows, :], bsend.at[s, g], brecv.at[s, g],
            me, lax.rem(z + way + Z, Z) * 2 + c,
        )

    def add_and_pass(g, s):
        way = way_of(g)
        rows = slice(g * GR, (g + 1) * GR)
        part = lax.rem(z - way * (1 + s) + 2 * Z, Z)
        total = pp_s[c, part, rows, :].astype(F32) + qb_s[part, rows, :].astype(F32)
        if s:
            pass_on(g, s - 1).wait_recv()
            total = total + rb_s[s - 1, rows, :].astype(F32)
        if s < Z - 1:
            pp_s[c, part, rows, :] = total.astype(BF16)
            pass_on(g, s).start()
        else:
            fs_s[rows, :] = total.astype(BF16)

    forward_group(0)
    order = [("relay", 1), ("ffn", 0)]
    hops = max(reach.values())
    for g in range(1, NG):
        order += [("forward", g)]
        if g + 1 <= hops:
            order += [("relay", g + 1)]
        order += [("ffn", g)]
    for hop in range(NG + 1, hops + 1):
        order += [("relay", hop)]
    for load in loads[6:]:
        load.wait()
    for what, n in order:
        if what == "relay":
            relay(n)
        elif what == "forward":
            forward_group(n)
        else:
            ffn(n)
    for g in range(NG):
        swap(g).wait_recv()
        add_and_pass(g, 0)

    def project(n):
        for r in range(Z) if n == 0 else ():
            share(r, pc).wait_recv()
        cols = slice(n * (TOK // 4), (n + 1) * (TOK // 4))
        outt = lax.dot_general(
            wo_s[...], m_s[:, cols], (((0,), (0,)), ((), ())), preferred_element_type=F32
        )
        out_s[cols, :] = outt.T.astype(BF16)

    def weigh(g):
        for k in range(g * KG, (g + 1) * KG):
            rows = slice(k * KR, (k + 1) * KR)
            gh_s[rows, :] = g_s[rows, :] * weight_hi[k : k + 1, :]
            gl_s[rows, :] = g_s[rows, :] * weight_lo[k : k + 1, :]

    side = [functools.partial(project, n) for n in range(4)] + [functools.partial(weigh, g) for g in range(NG)]
    out_copy = pltpu.make_async_copy(out_s, out_hbm, osem)
    for s in range(1, Z):
        for g in range(NG):
            add_and_pass(g, s)
        if s < Z - 1:
            for _ in range(-(-len(side) // max(1, Z - 1 - s))):
                side.pop(0)()
    out_copy.start()

    def give_back(k):
        rows = slice(k * KR, (k + 1) * KR)
        return remote(
            fs_s.at[rows, :], rr_s.at[rows, :], rsend.at[k], rrecv.at[k], moved(me, offs[k], E, back=True), t
        )

    for k in range(1, E):
        give_back(k).start()
    rr_s[0:KR, :] = fs_s[0:KR, :]
    for k in range(1, E):
        give_back(k).wait_recv()
    results = rr_s[...].T
    combined = jnp.dot(results, gh_s[...], preferred_element_type=F32) + jnp.dot(
        results, gl_s[...], preferred_element_type=F32
    )
    co_s[...] = combined.T.astype(BF16)

    def scatter(j):
        to = lax.rem(t + j, TP)
        return remote(
            co_s.at[pl.ds(pl.multiple_of(to * SUB, SUB), SUB), :], fo_s.at[t], zsend.at[j], zrecv.at[j], me, to
        )

    for j in range(1, TP):
        scatter(j).start()
    fo_s[t] = co_s[pl.ds(pl.multiple_of(t * SUB, SUB), SUB), :]
    for j in range(1, TP):
        source = lax.rem(t + TP - j, TP)
        remote(co_s.at[0:SUB, :], fo_s.at[source], zsend.at[j], zrecv.at[j], me, source).wait_recv()
    for j in range(TP):
        moe_ref[:, j * 128 : (j + 1) * 128] = fo_s[j]

    for k in range(1, E):
        dispatch(k).wait_send()
        hand_on(k).wait_send()
        give_back(k).wait_send()
    for k in range(E):
        forward(k).wait_send()
    for way, half in lanes:
        for hop in range(1, reach[way, half] + 1):
            ring(way, half, hop).wait_send()
    for r in range(Z):
        share(r, c).wait_send()
    for g in range(NG):
        swap(g).wait_send()
        for s in range(Z - 1):
            pass_on(g, s).wait_send()
    for j in range(1, TP):
        scatter(j).wait_send()
    out_copy.wait()


def on_device(
    query, forget, values, out_gate, gap, extra, head_gain, w_out,
    tokens, ff_gain, chosen, chosen_w, w_gate, w_up, w_down,
):
    E, TP = w_gate.shape[0] * lax.axis_size("ep"), lax.axis_size("tp")
    TOK, D = query.shape[0], tokens.shape[1]
    NTOK, FF = tokens.shape[0], w_gate.shape[2]
    SUB = NTOK // TP
    CAP = max(2, SUB * TOPK * 5 // (4 * E))
    Z, KR = TP // 2, TP * CAP
    ROWS, H = E * KR, D // 2
    KG = max(1, E // 4)
    NG = E // KG
    cfg = dict(E=E, TP=TP, TOK=TOK, SUB=SUB, CAP=CAP)
    any_spec = pl.BlockSpec(memory_space=pl.ANY)
    vmem = pl.BlockSpec(memory_space=pltpu.VMEM)
    dma = pltpu.SemaphoreType.DMA
    V = pltpu.VMEM
    hops = Z // 2
    return pl.pallas_call(
        functools.partial(kernel, cfg),
        out_shape=(
            jax.ShapeDtypeStruct((TOK, w_out.shape[1]), BF16),
            jax.ShapeDtypeStruct((SUB, D), BF16),
        ),
        in_specs=[any_spec] * 4 + [vmem] * 3 + [any_spec] * 2 + [vmem] * 3 + [any_spec] * 3,
        out_specs=(any_spec, vmem),
        scratch_shapes=[
            V((TOK, KEY_DIM), BF16), V((TOK, KEY_DIM), BF16), V((VAL_DIM, TOK), BF16), V((VAL_DIM, TOK), BF16),
            V(w_out.shape, BF16), V((2, NTOK, H), BF16), V((FF, D), BF16), V((FF, D), BF16), V((FF, D), BF16),
            V((PAIR, PAIR), F32), V((TOK // PAIR * 8, KEY_DIM), F32), V((TOK, KEY_DIM), F32),
            V((VAL_DIM, TOK), F32), V((TOK, KEY_DIM), BF16), V((VAL_DIM + 16, KEY_DIM), BF16),
            V((E, VAL_DIM + 16, KEY_DIM), BF16),
            V((NTOK, H), BF16), V((E, NTOK), F32), V((ROWS, NTOK), BF16), V((ROWS, H), BF16),
            V((2, ROWS, H), BF16), V((KG * KR, FF), BF16), V((2, Z, ROWS, 128), BF16),
            V((Z, ROWS, 128), BF16), V((Z - 1, ROWS, 128), BF16),
            V((TP * VAL_DIM, TOK), BF16), V((TOK, w_out.shape[1]), BF16), V((ROWS, 128), BF16),
            V((ROWS, 128), BF16), V((ROWS, NTOK), BF16), V((ROWS, NTOK), BF16), V((NTOK, 128), BF16),
            V((TP, SUB, 128), BF16),
            dma((10,)), dma, dma((E,)), dma((E,)), dma((E,)), dma((E,)), dma((E,)), dma((E,)),
            dma((2, 2, hops)), dma((2, 2, hops)), dma((Z,)), dma((Z,)), dma((NG,)), dma((NG,)),
            dma((Z - 1, NG)), dma((Z - 1, NG)), dma((E,)), dma((E,)), dma((TP,)), dma((TP,)),
        ],
        compiler_params=pltpu.CompilerParams(
            collective_id=0, has_side_effects=True, vmem_limit_bytes=64000 * 1024
        ),
    )(
        query, forget, values.T, out_gate.T, gap.reshape(1, -1), extra.T, head_gain.reshape(1, -1), w_out,
        tokens, ff_gain.reshape(1, -1), chosen.T, chosen_w.T, w_gate[0].T, w_up[0].T, w_down[0],
    )


def solution(mesh):
    placed = (
        P("ep", "tp"), P("ep", "tp"), P("ep", "tp"), P("ep", "tp"), P("tp"), P("ep", "tp"), P("tp"),
        P(None, "tp"), P("ep", None), P(), P("ep", None), P("ep", None),
        P("ep", None, "tp"), P("ep", None, "tp"), P("ep", "tp", None),
    )
    return jax.shard_map(
        on_device,
        mesh=mesh,
        in_specs=placed,
        out_specs=(P("ep", "tp"), P(("ep", "tp"), None)),
        check_vma=False,
    )
```

```python
import functools

import jax
import jax.numpy as jnp
from jax import lax
from jax.experimental import pallas as pl
from jax.experimental.pallas import tpu as pltpu
from jax.sharding import PartitionSpec as P

KEY_DIM = 128
VAL_DIM = 64
BLOCK = 64
PAIR = 128
TOPK = 2
EPS = 1e-06
MESH = pl.DeviceIdType.MESH
F32 = jnp.float32
BF16 = jnp.bfloat16
NT = (((1,), (1,)), ((), ()))


def offsets(experts):
    if experts == 16:
        return [
            (0, 0), (2, 2), (1, 2), (2, 1),
            (3, 2), (2, 3), (0, 2), (2, 0),
            (1, 1), (3, 3), (1, 3), (3, 1),
            (0, 1), (3, 0), (0, 3), (1, 0),
        ]
    return [(0, k) for k in range(experts)]


def moved(me, step, experts, back=False):
    dy, dx = step
    if experts != 16:
        return lax.rem(me + (experts - dx if back else dx), experts)
    y, x = me // 4, lax.rem(me, 4)
    if back:
        dy, dx = (4 - dy) % 4, (4 - dx) % 4
    return lax.rem(y + dy, 4) * 4 + lax.rem(x + dx, 4)


def kernel(
    cfg,
    q_hbm, f_hbm, v_hbm, o_hbm, gap_ref, extra_ref, hgain_ref, wo_hbm,
    x_hbm, fgain_ref, idx_ref, wt_ref, wg_hbm, wu_hbm, wd_hbm,
    out_hbm, moe_ref,
    q_s, f_s, v_s, o_s, wo_s, x_s, wg_s, wu_s, wd_s,
    tri_s, dec_s, pre_s, yw_s, qe_s, cs_s, cr_s,
    n_s, slot_s, g_s, s_s, r_s, hid_s, hp_s, pp_s, qb_s, rb_s,
    perm_s, perm_back_s, m_s, out_s, fs_s, fb_s, rr_s, gh_s, gl_s, co_s, mo_s,
    lsem, osem, asend, arecv, fsend, frecv, csend, crecv,
    msend, mrecv, dsend, drecv, psend, precv, bsend, brecv, rsend, rrecv, zsend, zrecv,
):
    E, TP, TOK, SUB, CAP = cfg["E"], cfg["TP"], cfg["TOK"], cfg["SUB"], cfg["CAP"]
    Z = TP // 2
    KR = TP * CAP
    KG = max(1, E // 4)
    NG = E // KG
    GR = KG * KR
    UNIT = 2 * CAP
    SG = max(1, E // 2)
    NS = E // SG
    SR = SG * UNIT
    D = x_hbm.shape[1]
    H = D // 2
    W = H // 2
    J = H // 128
    NTOK = x_hbm.shape[0]
    offs = offsets(E)
    me = lax.axis_index("ep")
    t = lax.axis_index("tp")
    z, c = t // 2, lax.rem(t, 2)
    pc = 1 - c

    def remote(src, dst, ss, rs, e, tt):
        return pltpu.make_async_remote_copy(
            src_ref=src, dst_ref=dst, send_sem=ss, recv_sem=rs, device_id=(e, tt), device_id_type=MESH
        )

    loads = [
        (x_hbm.at[:, 0:H], x_s.at[0]), (x_hbm.at[:, H:D], x_s.at[1]),
        (f_hbm, f_s), (q_hbm, q_s), (v_hbm, v_s), (o_hbm, o_s),
        (wg_hbm, wg_s), (wu_hbm, wu_s), (wd_hbm, wd_s), (wo_hbm, wo_s),
    ]
    loads = [pltpu.make_async_copy(a, b, lsem.at[i]) for i, (a, b) in enumerate(loads)]
    for load in loads:
        load.start()
    barrier = pltpu.get_barrier_semaphore()
    for k in range(1, E):
        pl.semaphore_signal(barrier, inc=1, device_id=(moved(me, offs[k], E), t), device_id_type=MESH)
    for j in (z * 2 + pc, lax.rem(z + 1, Z) * 2 + c, lax.rem(z + Z - 1, Z) * 2 + c):
        pl.semaphore_signal(barrier, inc=1, device_id=(me, j), device_id_type=MESH)

    i0, i1 = idx_ref[0:1, :], idx_ref[1:2, :]
    row_e = lax.broadcasted_iota(jnp.int32, (E, NTOK), 0)
    expert_of = jnp.zeros((E, NTOK), jnp.int32)
    for k in range(E):
        expert_of = jnp.where(row_e == k, moved(me, offs[k], E), expert_of)
    first, second = expert_of == i0, expert_of == i1
    chosen = jnp.where(first | second, 1.0, 0.0)
    ra = lax.broadcasted_iota(jnp.int32, (NTOK, NTOK), 0)
    rb = lax.broadcasted_iota(jnp.int32, (NTOK, NTOK), 1)
    before = jnp.where((ra // SUB == rb // SUB) & (ra < rb), 1.0, 0.0).astype(BF16)
    place = jnp.dot(chosen.astype(BF16), before, preferred_element_type=F32)
    block_of = (lax.broadcasted_iota(jnp.int32, (E, NTOK), 1) // SUB).astype(F32)
    slot_s[...] = jnp.where(chosen > 0, CAP * block_of + place, -1.0)
    weight = jnp.where(first, wt_ref[0:1, :], 0.0) + jnp.where(second, wt_ref[1:2, :], 0.0)
    weight_hi = weight.astype(BF16)
    weight_lo = (weight - weight_hi.astype(F32)).astype(BF16)

    loads[0].wait()
    loads[1].wait()
    gain_half = fgain_ref[:, pl.ds(pl.multiple_of(c * H, 128), H)]

    def norm_rows(i, carry):
        rows = pl.ds(pl.multiple_of(i * 64, 64), 64)
        a, b = x_s[0, rows, :].astype(F32), x_s[1, rows, :].astype(F32)
        total = jnp.sum(a * a + b * b, axis=-1, keepdims=True)
        factor = lax.rsqrt(total / D + EPS)
        n_s[rows, :] = (x_s[c, rows, :].astype(F32) * factor * gain_half).astype(BF16)
        return carry

    lax.fori_loop(0, NTOK // 64, norm_rows, 0)

    place_row = lax.broadcasted_iota(jnp.int32, (KR, NTOK), 0).astype(F32)

    def fill_group(g):
        for k in range(g * KG, (g + 1) * KG):
            rows = slice(k * KR, (k + 1) * KR)
            g_s[rows, :] = jnp.where(place_row == slot_s[k : k + 1, :], 1.0, 0.0).astype(BF16)
        rows = slice(g * GR, (g + 1) * GR)
        pick = g_s[rows, :]
        for n in range(0, H, 256):
            s_s[rows, n : n + 256] = jnp.dot(
                pick, n_s[:, n : n + 256], preferred_element_type=F32
            ).astype(BF16)

    def dispatch(k):
        rows = slice(k * KR, (k + 1) * KR)
        return remote(
            s_s.at[rows, :], r_s.at[c, rows, :], asend.at[k], arecv.at[k], moved(me, offs[k], E), t
        )

    def forward(k):
        rows = slice(k * KR, (k + 1) * KR)
        return remote(
            r_s.at[c, rows, :], r_s.at[c, rows, :], fsend.at[k], frecv.at[k], me, z * 2 + pc
        )

    fill_group(0)
    r_s[c, 0:KR, :] = s_s[0:KR, :]

    ta = lax.broadcasted_iota(jnp.int32, (PAIR, PAIR), 0)
    tb = lax.broadcasted_iota(jnp.int32, (PAIR, PAIR), 1)
    tri = (ta // BLOCK == tb // BLOCK) & (ta >= tb)
    tri_s[...] = jnp.where(tri, 1.0, 0.0)
    gap = gap_ref[...]
    for load in loads[2:6]:
        load.wait()
    U1 = min(4, TOK // PAIR)

    def local_pairs(i, carry):
        state, decay = carry
        trif = tri_s[...]
        trib = trif.astype(BF16)
        in_first = lax.broadcasted_iota(jnp.int32, (PAIR, PAIR), 0) < BLOCK
        left = lax.broadcasted_iota(jnp.int32, (BLOCK, PAIR), 1) < BLOCK
        later = lax.broadcasted_iota(jnp.int32, (PAIR, PAIR), 1)
        earlier = lax.broadcasted_iota(jnp.int32, (PAIR, PAIR), 0)
        maskt = (later // BLOCK == earlier // BLOCK) & (earlier <= later)
        at = [pl.multiple_of((i * U1 + u) * PAIR, PAIR) for u in range(U1)]
        keys, cums = [], []
        for u in range(U1):
            gate = f_s[pl.ds(at[u], PAIR), :].astype(F32)
            key = gap * (1.0 / (1.0 + jnp.exp(gate)))
            logf = jnp.log(1.0 - key)
            hi = logf.astype(BF16)
            lo = (logf - hi.astype(F32)).astype(BF16)
            cum = jnp.dot(trib, hi, preferred_element_type=F32) + jnp.dot(
                trib, lo, preferred_element_type=F32
            )
            extra = jnp.sum(trif * extra_ref[:, pl.ds(at[u], PAIR)], axis=-1, keepdims=True)
            keys.append(key)
            cums.append(cum + extra)
        work = []
        for u in range(U1):
            key, cum = keys[u], cums[u]
            mid0, mid1 = cum[31:32, :], cum[95:96, :]
            end0, end1 = cum[63:64, :], cum[127:128, :]
            away = cum - jnp.where(in_first, mid0, mid1)
            query = q_s[pl.ds(at[u], PAIR), :].astype(F32)
            query = query * (1.0 / (1.0 + jnp.exp(-query)))
            qs = query * jnp.exp(away)
            ks = key * jnp.exp(-away)
            qe = qs * jnp.where(in_first, jnp.exp(mid0), jnp.exp(mid1))
            ke = ks * jnp.where(in_first, jnp.exp(end0 - mid0), jnp.exp(end1 - mid1))
            qe_s[pl.ds(at[u], PAIR), :] = qe.astype(BF16)
            work.append((qs.astype(BF16), ks.astype(BF16), ke.astype(BF16), jnp.exp(end0), jnp.exp(end1)))
        scores = [lax.dot_general(w[1], w[0], NT, preferred_element_type=F32) for w in work]
        updates = []
        for u in range(U1):
            vt = v_s[:, pl.ds(at[u], PAIR)]
            both = jnp.where(maskt, scores[u], 0.0).astype(BF16)
            yw_s[:, pl.ds(at[u], PAIR)] = jnp.dot(vt, both, preferred_element_type=F32)
            zero = jnp.zeros_like(vt)
            split = jnp.concatenate([jnp.where(left, vt, zero), jnp.where(left, zero, vt)], axis=0)
            updates.append(jnp.dot(split, work[u][2], preferred_element_type=F32))
        for u in range(U1):
            d0, d1 = work[u][3], work[u][4]
            middle = d0 * state + updates[u][0:BLOCK, :]
            pre_s[pl.ds(at[u], BLOCK), :] = state
            pre_s[pl.ds(pl.multiple_of(at[u] + BLOCK, BLOCK), BLOCK), :] = middle
            half = decay * d0
            dec_s[pl.ds(pl.multiple_of((i * U1 + u) * 8, 8), 8), :] = jnp.concatenate(
                [decay, half, jnp.zeros((6, KEY_DIM), F32)], axis=0
            )
            state = d1 * middle + updates[u][BLOCK:PAIR, :]
            decay = half * d1
        return state, decay

    state, decay = lax.fori_loop(
        0, TOK // (PAIR * U1), local_pairs,
        (jnp.zeros((VAL_DIM, KEY_DIM), F32), jnp.ones((1, KEY_DIM), F32)),
    )
    decay_hi = decay.astype(BF16).astype(F32)
    row16 = lax.broadcasted_iota(jnp.int32, (16, KEY_DIM), 0)
    tail = jnp.where(row16 == 0, decay_hi, jnp.where(row16 == 1, decay - decay_hi, 0.0))
    cs_s[0:VAL_DIM, :] = state.astype(BF16)
    cs_s[VAL_DIM : VAL_DIM + 16, :] = tail.astype(BF16)
    cr_s[me] = jnp.zeros((VAL_DIM + 16, KEY_DIM), BF16)

    def hand_on(k):
        return remote(cs_s, cr_s.at[me], csend.at[k], crecv.at[me], moved(me, offs[k], E), t)

    def handed(k):
        source = moved(me, offs[k], E, back=True)
        return remote(cs_s, cr_s.at[source], csend.at[k], crecv.at[source], source, t)

    pl.semaphore_wait(barrier, E - 1 + 3)
    for k in range(1, E):
        hand_on(k).start()
    for k in range(1, KG):
        dispatch(k).start()
    for g in range(1, NG):
        fill_group(g)
        for k in range(g * KG, (g + 1) * KG):
            dispatch(k).start()

    def swapper(ref, outer, inner):
        size = outer * inner * UNIT
        row = lax.broadcasted_iota(jnp.int32, (size, 1), 0)
        source = (row // UNIT % inner * outer + row // (inner * UNIT)) * UNIT + row % UNIT
        ref[...] = jnp.where(lax.broadcasted_iota(jnp.int32, (size, size), 1) == source, 1.0, 0.0).astype(BF16)

    swapper(perm_s, Z, SG)
    swapper(perm_back_s, SG, J)

    for k in range(1, E):
        handed(k).wait_recv()
    start = jnp.zeros((VAL_DIM, KEY_DIM), F32)
    for j in range(E - 1):
        ends = cr_s[j, VAL_DIM : VAL_DIM + 16, :].astype(F32)
        after = (ends[0:1, :] + ends[1:2, :]) * start + cr_s[j, 0:VAL_DIM, :].astype(F32)
        start = jnp.where(j < me, after, start)
    ga = lax.broadcasted_iota(jnp.int32, (VAL_DIM, VAL_DIM), 0)
    gb = lax.broadcasted_iota(jnp.int32, (VAL_DIM, VAL_DIM), 1)
    head_gain = jnp.sum(jnp.where(ga == gb, hgain_ref[...], 0.0), axis=-1, keepdims=True)
    own_rows = pl.multiple_of(t * VAL_DIM, VAL_DIM)

    def finish_pairs(i, carry):
        left = lax.broadcasted_iota(jnp.int32, (BLOCK, PAIR), 1) < BLOCK
        at = [pl.multiple_of((i * U1 + u) * PAIR, PAIR) for u in range(U1)]
        across = []
        for u in range(U1):
            d = dec_s[pl.ds(pl.multiple_of((i * U1 + u) * 8, 8), 8), :]
            s0 = pre_s[pl.ds(at[u], BLOCK), :] + d[0:1, :] * start
            s1 = pre_s[pl.ds(pl.multiple_of(at[u] + BLOCK, BLOCK), BLOCK), :] + d[1:2, :] * start
            states = jnp.concatenate([s0, s1], axis=0).astype(BF16)
            across.append(
                lax.dot_general(states, qe_s[pl.ds(at[u], PAIR), :], NT, preferred_element_type=F32)
            )
        for u in range(U1):
            cols = pl.ds(at[u], PAIR)
            y = yw_s[:, cols] + jnp.where(left, across[u][0:BLOCK, :], across[u][BLOCK:PAIR, :])
            factor = lax.rsqrt(jnp.mean(y * y, axis=0, keepdims=True) + EPS)
            gate = o_s[:, cols].astype(F32)
            gate = gate * (1.0 / (1.0 + jnp.exp(-gate)))
            m_s[pl.ds(own_rows, VAL_DIM), cols] = (y * factor * head_gain * gate).astype(BF16)
        return carry

    lax.fori_loop(0, TOK // (PAIR * U1), finish_pairs, 0)

    VH = VAL_DIM // 2
    reach = {(1, 0): Z // 2, (1, 1): Z - 1 - Z // 2, (-1, 0): Z - 1 - Z // 2, (-1, 1): Z // 2}

    def head_at(zz, core):
        return pl.multiple_of((lax.rem(zz + 2 * Z, Z) * 2 + core) * VAL_DIM, VAL_DIM)

    def ring(way, half, hop):
        rows = pl.ds(pl.multiple_of(head_at(z - way * (hop - 1), c) + half * VH, VH), VH)
        w = 0 if way == 1 else 1
        return remote(
            m_s.at[rows, :], m_s.at[rows, :], msend.at[w, half, hop - 1], mrecv.at[w, half, hop - 1],
            me, lax.rem(z + way + Z, Z) * 2 + c,
        )

    def ringed(way, half, hop):
        rows = pl.ds(pl.multiple_of(head_at(z - way * hop, c) + half * VH, VH), VH)
        w = 0 if way == 1 else 1
        return remote(
            m_s.at[rows, :], m_s.at[rows, :], msend.at[w, half, hop - 1], mrecv.at[w, half, hop - 1],
            me, lax.rem(z + way + Z, Z) * 2 + c,
        )

    def share(r, core):
        rows = pl.ds(head_at(z - r, core), VAL_DIM)
        return remote(m_s.at[rows, :], m_s.at[rows, :], dsend.at[r], drecv.at[r], me, z * 2 + pc)

    lanes = [(1, 0), (-1, 1), (1, 1), (-1, 0)]

    def relay(hop):
        for way, half in lanes:
            if hop <= reach[way, half]:
                ringed(way, half, hop).wait_recv()
                if hop + 1 <= reach[way, half]:
                    ring(way, half, hop + 1).start()
        if hop == Z - hop:
            share(hop, c).start()
        elif hop < Z - hop:
            share(hop, c).start()
            share(Z - hop, c).start()

    for way, half in lanes:
        if reach[way, half] >= 1:
            ring(way, half, 1).start()
    share(0, c).start()

    def forward_group(g):
        for k in range(g * KG, (g + 1) * KG):
            if k:
                dispatch(k).wait_recv()
            forward(k).start()

    def ffn(g):
        rows = slice(g * GR, (g + 1) * GR)
        for k in range(g * KG, (g + 1) * KG):
            back = slice(k * KR, (k + 1) * KR)
            remote(
                r_s.at[c, back, :], r_s.at[pc, back, :], fsend.at[k], frecv.at[k], me, z * 2 + pc
            ).wait_recv()
        a, b = r_s[0, rows, :], r_s[1, rows, :]
        gate = lax.dot_general(a, wg_s[:, 0:H], NT, preferred_element_type=F32) + lax.dot_general(
            b, wg_s[:, H:D], NT, preferred_element_type=F32
        )
        up = lax.dot_general(a, wu_s[:, 0:H], NT, preferred_element_type=F32) + lax.dot_general(
            b, wu_s[:, H:D], NT, preferred_element_type=F32
        )
        hid_s[rows, :] = (gate * (1.0 / (1.0 + jnp.exp(-gate))) * up).astype(BF16)

    def relative(r):
        return lax.rem(z + r + 2 * Z, Z)

    def swap(g, r):
        part = relative(r)
        return remote(
            pp_s.at[pc, :, g, part], qb_s.at[:, g, part], psend.at[g, r % Z], precv.at[g, r % Z],
            me, z * 2 + pc,
        )

    def pass_on(g, d, s):
        way = 1 - 2 * d
        part = relative(-way * (1 + s))
        return remote(
            pp_s.at[c, d, g, part], rb_s.at[s, g, d], bsend.at[s, g, d], brecv.at[s, g, d],
            me, relative(way) * 2 + c,
        )

    swapped = set()

    def add_and_pass(g, d, s):
        r = -(1 - 2 * d) * (1 + s)
        part = relative(r)
        if (g, r % Z) not in swapped:
            swapped.add((g, r % Z))
            swap(g, r).wait_recv()
        total = pp_s[c, d, g, part].astype(F32) + qb_s[d, g, part].astype(F32)
        if s:
            pass_on(g, d, s - 1).wait_recv()
            total = total + rb_s[s - 1, g, d].astype(F32)
        if s < Z - 1:
            pp_s[c, d, g, part] = total.astype(BF16)
            pass_on(g, d, s).start()
        else:
            for n in range(W // 128):
                at = (d * (W // 128) + n) * SR
                fs_s[g, at : at + SR, :] = total[:, n * 128 : n * 128 + 128].astype(BF16)

    def down(g):
        rows = slice(g * Z * SR, (g + 1) * Z * SR)
        hp_s[rows, :] = jnp.dot(
            perm_s[...], hid_s[rows, :], preferred_element_type=F32
        ).astype(BF16)
        turns = [r for n in range(1, Z // 2) for r in (-n, n)] + [Z // 2, 0]
        for n in range(0, Z, 2):
            pair = turns[n : n + 2]
            hid = jnp.concatenate(
                [
                    hp_s[pl.ds(pl.multiple_of((g * Z + relative(r)) * SR, 16), SR), :]
                    for r in pair
                ],
                axis=0,
            )
            for half in range(2):
                for d in range(2):
                    cols = slice(half * H + d * W, half * H + (d + 1) * W)
                    y = jnp.dot(hid, wd_s[:, cols], preferred_element_type=F32).astype(BF16)
                    for i, r in enumerate(pair):
                        pp_s[half, d, g, relative(r)] = y[i * SR : (i + 1) * SR, :]
            for r in pair:
                swap(g, r).start()
            if n == min(2, Z - 2):
                for d in range(2):
                    add_and_pass(g, d, 0)

    hops = max(reach.values())
    for load in loads[6:]:
        load.wait()
    forward_group(0)
    done = 0
    for g in range(NG):
        ffn(g)
        if g + 1 < NG:
            forward_group(g + 1)
        if g + 1 <= hops:
            relay(g + 1)
        while done < NS and (done + 1) * SG <= (g + 1) * KG:
            down(done)
            done += 1
    for hop in range(NG + 1, hops + 1):
        relay(hop)

    out_copy = pltpu.make_async_copy(out_s, out_hbm, osem)

    def project(n):
        for r in range(Z) if n == 0 else ():
            share(r, pc).wait_recv()
        cols = slice(n * (TOK // 4), (n + 1) * (TOK // 4))
        outt = lax.dot_general(
            wo_s[...], m_s[:, cols], (((0,), (0,)), ((), ())), preferred_element_type=F32
        )
        out_s[cols, :] = outt.T.astype(BF16)
        if n == 3:
            out_copy.start()

    lanes_out = J * 2 * SUB
    lane = lax.broadcasted_iota(jnp.int32, (1, lanes_out), 1)

    def weigh_all():
        token = lax.broadcasted_iota(jnp.int32, (NTOK, lanes_out), 0)
        mine = z * 2 * SUB + lane % (2 * SUB)
        pick = jnp.where(token == mine, 1.0, 0.0).astype(BF16)
        local = slot_s[...] - (z * UNIT).astype(F32)
        local = jnp.where((local >= 0) & (local < UNIT), local, -1.0).astype(BF16)
        place_at = jnp.dot(local, pick, preferred_element_type=F32)
        high = jnp.dot(weight_hi, pick, preferred_element_type=F32)
        low = jnp.dot(weight_lo, pick, preferred_element_type=F32)
        shift = (lane // (2 * SUB) * UNIT).astype(F32)
        target = jnp.where(place_at >= 0, place_at + shift, -1.0)
        row = lax.broadcasted_iota(jnp.int32, (J * UNIT, lanes_out), 0).astype(F32)
        for k in range(E):
            rows = slice(k * J * UNIT, (k + 1) * J * UNIT)
            here = row == target[k : k + 1, :]
            gh_s[rows, :] = jnp.where(here, high[k : k + 1, :], 0.0).astype(BF16)
            gl_s[rows, :] = jnp.where(here, low[k : k + 1, :], 0.0).astype(BF16)

    BR = J * UNIT

    def give_back(k):
        rows = slice(k * BR, (k + 1) * BR)
        return remote(
            fb_s.at[rows, :], rr_s.at[rows, :], rsend.at[k], rrecv.at[k], moved(me, offs[k], E, back=True), t
        )

    side = [functools.partial(project, n) for n in range(4)] + [weigh_all]
    for s in range(1, Z):
        for g in range(NS):
            for d in range(2):
                add_and_pass(g, d, s)
            if s == Z - 1:
                rows = slice(g * SG * BR, (g + 1) * SG * BR)
                fb_s[rows, :] = jnp.dot(
                    perm_back_s[...], fs_s[g], preferred_element_type=F32
                ).astype(BF16)
                for k in range(g * SG, (g + 1) * SG):
                    if k:
                        give_back(k).start()
        if s < Z - 1:
            for _ in range(-(-len(side) // max(1, Z - 1 - s))):
                side.pop(0)()
    while side:
        side.pop(0)()
    rr_s[0:BR, :] = fb_s[0:BR, :]
    for k in range(1, E):
        give_back(k).wait_recv()
    results = rr_s[...].T
    combined = jnp.dot(results, gh_s[...], preferred_element_type=F32) + jnp.dot(
        results, gl_s[...], preferred_element_type=F32
    )
    combined = combined.T.astype(BF16)
    for j in range(J):
        co_s[j] = combined[j * 2 * SUB : (j + 1) * 2 * SUB, :]

    def hand_over(core):
        mine = pl.ds(pl.multiple_of((1 - core) * SUB, SUB), SUB)
        return remote(co_s.at[:, mine, :], mo_s.at[core], zsend, zrecv, me, z * 2 + pc)

    hand_over(c).start()
    mo_s[c] = co_s[:, pl.ds(pl.multiple_of(c * SUB, SUB), SUB), :]
    hand_over(pc).wait_recv()
    for half in range(2):
        for j in range(J):
            moe_ref[:, half * H + j * 128 : half * H + (j + 1) * 128] = mo_s[half, j]

    for k in range(1, E):
        dispatch(k).wait_send()
        hand_on(k).wait_send()
        give_back(k).wait_send()
    for k in range(E):
        forward(k).wait_send()
    for way, half in lanes:
        for hop in range(1, reach[way, half] + 1):
            ring(way, half, hop).wait_send()
    for r in range(Z):
        share(r, c).wait_send()
    for g in range(NS):
        for r in range(Z):
            swap(g, r).wait_send()
        for d in range(2):
            for s in range(Z - 1):
                pass_on(g, d, s).wait_send()
    hand_over(c).wait_send()
    out_copy.wait()


def on_device(
    query, forget, values, out_gate, gap, extra, head_gain, w_out,
    tokens, ff_gain, chosen, chosen_w, w_gate, w_up, w_down,
):
    E, TP = w_gate.shape[0] * lax.axis_size("ep"), lax.axis_size("tp")
    TOK, D = query.shape[0], tokens.shape[1]
    NTOK, FF = tokens.shape[0], w_gate.shape[2]
    SUB = NTOK // TP
    CAP = max(2, SUB * TOPK * 5 // (4 * E))
    Z, KR = TP // 2, TP * CAP
    ROWS, H = E * KR, D // 2
    KG = max(1, E // 4)
    NG = E // KG
    SG = max(1, E // 2)
    NS, UNIT, J = E // SG, 2 * CAP, H // 128
    SR = SG * UNIT
    cfg = dict(E=E, TP=TP, TOK=TOK, SUB=SUB, CAP=CAP)
    any_spec = pl.BlockSpec(memory_space=pl.ANY)
    vmem = pl.BlockSpec(memory_space=pltpu.VMEM)
    dma = pltpu.SemaphoreType.DMA
    V = pltpu.VMEM
    hops = Z // 2
    return pl.pallas_call(
        functools.partial(kernel, cfg),
        out_shape=(
            jax.ShapeDtypeStruct((TOK, w_out.shape[1]), BF16),
            jax.ShapeDtypeStruct((SUB, D), BF16),
        ),
        in_specs=[any_spec] * 4 + [vmem] * 3 + [any_spec] * 2 + [vmem] * 3 + [any_spec] * 3,
        out_specs=(any_spec, vmem),
        scratch_shapes=[
            V((TOK, KEY_DIM), BF16), V((TOK, KEY_DIM), BF16), V((VAL_DIM, TOK), BF16), V((VAL_DIM, TOK), BF16),
            V(w_out.shape, BF16), V((2, NTOK, H), BF16), V((FF, D), BF16), V((FF, D), BF16), V((FF, D), BF16),
            V((PAIR, PAIR), F32), V((TOK // PAIR * 8, KEY_DIM), F32), V((TOK, KEY_DIM), F32),
            V((VAL_DIM, TOK), F32), V((TOK, KEY_DIM), BF16), V((VAL_DIM + 16, KEY_DIM), BF16),
            V((E, VAL_DIM + 16, KEY_DIM), BF16),
            V((NTOK, H), BF16), V((E, NTOK), F32), V((ROWS, NTOK), BF16), V((ROWS, H), BF16),
            V((2, ROWS, H), BF16), V((ROWS, FF), BF16), V((ROWS, FF), BF16),
            V((2, 2, NS, Z, SR, H // 2), BF16), V((2, NS, Z, SR, H // 2), BF16), V((Z - 1, NS, 2, SR, H // 2), BF16),
            V((Z * SR, Z * SR), BF16), V((J * SR, J * SR), BF16),
            V((TP * VAL_DIM, TOK), BF16), V((TOK, w_out.shape[1]), BF16), V((NS, J * SR, 128), BF16),
            V((E * J * UNIT, 128), BF16), V((E * J * UNIT, 128), BF16),
            V((E * J * UNIT, J * 2 * SUB), BF16), V((E * J * UNIT, J * 2 * SUB), BF16),
            V((J, 2 * SUB, 128), BF16), V((2, J, SUB, 128), BF16),
            dma((10,)), dma, dma((E,)), dma((E,)), dma((E,)), dma((E,)), dma((E,)), dma((E,)),
            dma((2, 2, hops)), dma((2, 2, hops)), dma((Z,)), dma((Z,)), dma((NS, Z)), dma((NS, Z)),
            dma((Z - 1, NS, 2)), dma((Z - 1, NS, 2)), dma((E,)), dma((E,)), dma, dma,
        ],
        compiler_params=pltpu.CompilerParams(
            collective_id=0, has_side_effects=True, vmem_limit_bytes=64000 * 1024
        ),
    )(
        query, forget, values.T, out_gate.T, gap.reshape(1, -1), extra.T, head_gain.reshape(1, -1), w_out,
        tokens, ff_gain.reshape(1, -1), chosen.T, chosen_w.T, w_gate[0].T, w_up[0].T, w_down[0],
    )


def solution(mesh):
    placed = (
        P("ep", "tp"), P("ep", "tp"), P("ep", "tp"), P("ep", "tp"), P("tp"), P("ep", "tp"), P("tp"),
        P(None, "tp"), P("ep", None), P(), P("ep", None), P("ep", None),
        P("ep", None, "tp"), P("ep", None, "tp"), P("ep", "tp", None),
    )
    return jax.shard_map(
        on_device,
        mesh=mesh,
        in_specs=placed,
        out_specs=(P("ep", "tp"), P(("ep", "tp"), None)),
        check_vma=False,
    )
```

```python
import functools

import jax
import jax.numpy as jnp
from jax import lax
from jax.experimental import pallas as pl
from jax.experimental.pallas import tpu as pltpu
from jax.sharding import PartitionSpec as P

KEY_DIM = 128
VAL_DIM = 64
BLOCK = 64
PAIR = 128
TOPK = 2
EPS = 1e-06
MESH = pl.DeviceIdType.MESH
F32 = jnp.float32
BF16 = jnp.bfloat16
NT = (((1,), (1,)), ((), ()))


def offsets(experts):
    if experts == 16:
        return [
            (0, 0), (2, 2), (1, 2), (2, 1),
            (3, 2), (2, 3), (0, 1), (3, 0),
            (1, 1), (3, 3), (0, 2), (2, 0),
            (1, 3), (3, 1), (0, 3), (1, 0),
        ]
    return [(0, k) for k in range(experts)]


def moved(me, step, experts, back=False):
    dy, dx = step
    if experts != 16:
        return lax.rem(me + (experts - dx if back else dx), experts)
    y, x = me // 4, lax.rem(me, 4)
    if back:
        dy, dx = (4 - dy) % 4, (4 - dx) % 4
    return lax.rem(y + dy, 4) * 4 + lax.rem(x + dx, 4)


def kernel(
    cfg,
    q_hbm, f_hbm, v_hbm, o_hbm, gap_ref, extra_ref, hgain_ref, wo_hbm,
    x_hbm, fgain_ref, idx_ref, wt_ref, wg_hbm, wu_hbm, wd_hbm,
    out_hbm, moe_ref,
    q_s, f_s, v_s, o_s, wo_s, x_s, wg_s, wu_s, wd_s,
    tri_s, dec_s, pre_s, yw_s, qe_s, cs_s, cr_s,
    n_s, slot_s, g_s, s_s, r_s, ga_s, ua_s, hid_s, hp_s, pp_s, qb_s, rb_s,
    perm_s, perm_back_s, m_s, out_s, fs_s, fb_s, rr_s, gh_s, gl_s, co_s, mo_s,
    lsem, osem, asend, arecv, fsend, frecv, csend, crecv,
    msend, mrecv, dsend, drecv, psend, precv, bsend, brecv, rsend, rrecv, zsend, zrecv,
):
    E, TP, TOK, SUB, CAP = cfg["E"], cfg["TP"], cfg["TOK"], cfg["SUB"], cfg["CAP"]
    Z = TP // 2
    KR = TP * CAP
    KG = max(1, E // 4)
    NG = E // KG
    GR = KG * KR
    UNIT = 2 * CAP
    SG = max(1, E // 2)
    NS = E // SG
    SR = SG * UNIT
    D = x_hbm.shape[1]
    H = D // 2
    ND = cfg["ND"]
    W = H // ND
    NW = cfg["NW"]
    HW = H // NW
    J = H // 128
    NTOK = x_hbm.shape[0]
    offs = offsets(E)
    me = lax.axis_index("ep")
    t = lax.axis_index("tp")
    z, c = t // 2, lax.rem(t, 2)
    pc = 1 - c

    def remote(src, dst, ss, rs, e, tt):
        return pltpu.make_async_remote_copy(
            src_ref=src, dst_ref=dst, send_sem=ss, recv_sem=rs, device_id=(e, tt), device_id_type=MESH
        )

    loads = [
        (f_hbm, f_s), (q_hbm, q_s), (v_hbm, v_s), (x_hbm.at[:, 0:H], x_s.at[0]), (x_hbm.at[:, H:D], x_s.at[1]),
        (o_hbm, o_s),
        (wg_hbm, wg_s), (wu_hbm, wu_s), (wd_hbm, wd_s), (wo_hbm, wo_s),
    ]
    loads = [pltpu.make_async_copy(a, b, lsem.at[i]) for i, (a, b) in enumerate(loads)]
    for load in loads:
        load.start()
    barrier = pltpu.get_barrier_semaphore()
    for k in range(1, E):
        pl.semaphore_signal(barrier, inc=1, device_id=(moved(me, offs[k], E), t), device_id_type=MESH)
    for j in (z * 2 + pc, lax.rem(z + 1, Z) * 2 + c, lax.rem(z + Z - 1, Z) * 2 + c):
        pl.semaphore_signal(barrier, inc=1, device_id=(me, j), device_id_type=MESH)

    i0, i1 = idx_ref[0:1, :], idx_ref[1:2, :]
    row_e = lax.broadcasted_iota(jnp.int32, (E, NTOK), 0)
    expert_of = jnp.zeros((E, NTOK), jnp.int32)
    for k in range(E):
        expert_of = jnp.where(row_e == k, moved(me, offs[k], E), expert_of)
    first, second = expert_of == i0, expert_of == i1
    chosen = jnp.where(first | second, 1.0, 0.0)
    ra = lax.broadcasted_iota(jnp.int32, (NTOK, NTOK), 0)
    rb = lax.broadcasted_iota(jnp.int32, (NTOK, NTOK), 1)
    before = jnp.where((ra // SUB == rb // SUB) & (ra < rb), 1.0, 0.0).astype(BF16)
    place = jnp.dot(chosen.astype(BF16), before, preferred_element_type=F32)
    block_of = (lax.broadcasted_iota(jnp.int32, (E, NTOK), 1) // SUB).astype(F32)
    slot_s[...] = jnp.where(chosen > 0, CAP * block_of + place, -1.0)
    weight = jnp.where(first, wt_ref[0:1, :], 0.0) + jnp.where(second, wt_ref[1:2, :], 0.0)
    weight_hi = weight.astype(BF16)
    weight_lo = (weight - weight_hi.astype(F32)).astype(BF16)

    place_row = lax.broadcasted_iota(jnp.int32, (KR, NTOK), 0).astype(F32)

    def fill_group(g):
        for k in range(g * KG, (g + 1) * KG):
            rows = slice(k * KR, (k + 1) * KR)
            g_s[rows, :] = jnp.where(place_row == slot_s[k : k + 1, :], 1.0, 0.0).astype(BF16)
        rows = slice(g * GR, (g + 1) * GR)
        pick = g_s[rows, :]
        for n in range(0, H, min(HW, 256)):
            at = n % HW
            s_s[n // HW, rows, at : at + min(HW, 256)] = jnp.dot(
                pick, n_s[:, n : n + min(HW, 256)], preferred_element_type=F32
            ).astype(BF16)

    def dispatch(w, k):
        rows = slice(k * KR, (k + 1) * KR)
        return remote(
            s_s.at[w, rows, :], r_s.at[c, w, rows, :], asend.at[w, k], arecv.at[w, k],
            moved(me, offs[k], E), t,
        )

    def forward(w, g, core):
        rows = slice(g * GR, (g + 1) * GR)
        return remote(
            r_s.at[core, w, rows, :], r_s.at[core, w, rows, :], fsend.at[w, g], frecv.at[w, g], me, z * 2 + pc
        )

    ta = lax.broadcasted_iota(jnp.int32, (PAIR, PAIR), 0)
    tb = lax.broadcasted_iota(jnp.int32, (PAIR, PAIR), 1)
    tri = (ta // BLOCK == tb // BLOCK) & (ta >= tb)
    tri_s[...] = jnp.where(tri, 1.0, 0.0)
    gap = gap_ref[...]
    for load in loads[0:3]:
        load.wait()
    U1 = min(4, TOK // PAIR)

    def local_pairs(i, carry):
        state, decay = carry
        trif = tri_s[...]
        trib = trif.astype(BF16)
        in_first = lax.broadcasted_iota(jnp.int32, (PAIR, PAIR), 0) < BLOCK
        left = lax.broadcasted_iota(jnp.int32, (BLOCK, PAIR), 1) < BLOCK
        later = lax.broadcasted_iota(jnp.int32, (PAIR, PAIR), 1)
        earlier = lax.broadcasted_iota(jnp.int32, (PAIR, PAIR), 0)
        maskt = (later // BLOCK == earlier // BLOCK) & (earlier <= later)
        at = [pl.multiple_of((i * U1 + u) * PAIR, PAIR) for u in range(U1)]
        keys, cums = [], []
        for u in range(U1):
            gate = f_s[pl.ds(at[u], PAIR), :].astype(F32)
            key = gap * (1.0 / (1.0 + jnp.exp(gate)))
            logf = jnp.log(1.0 - key)
            hi = logf.astype(BF16)
            lo = (logf - hi.astype(F32)).astype(BF16)
            cum = jnp.dot(trib, hi, preferred_element_type=F32) + jnp.dot(
                trib, lo, preferred_element_type=F32
            )
            extra = jnp.sum(trif * extra_ref[:, pl.ds(at[u], PAIR)], axis=-1, keepdims=True)
            keys.append(key)
            cums.append(cum + extra)
        work = []
        for u in range(U1):
            key, cum = keys[u], cums[u]
            mid0, mid1 = cum[31:32, :], cum[95:96, :]
            end0, end1 = cum[63:64, :], cum[127:128, :]
            away = cum - jnp.where(in_first, mid0, mid1)
            query = q_s[pl.ds(at[u], PAIR), :].astype(F32)
            query = query * (1.0 / (1.0 + jnp.exp(-query)))
            qs = query * jnp.exp(away)
            ks = key * jnp.exp(-away)
            qe = qs * jnp.where(in_first, jnp.exp(mid0), jnp.exp(mid1))
            ke = ks * jnp.where(in_first, jnp.exp(end0 - mid0), jnp.exp(end1 - mid1))
            qe_s[pl.ds(at[u], PAIR), :] = qe.astype(BF16)
            work.append((qs.astype(BF16), ks.astype(BF16), ke.astype(BF16), jnp.exp(end0), jnp.exp(end1)))
        scores = [lax.dot_general(w[1], w[0], NT, preferred_element_type=F32) for w in work]
        updates = []
        for u in range(U1):
            vt = v_s[:, pl.ds(at[u], PAIR)]
            both = jnp.where(maskt, scores[u], 0.0).astype(BF16)
            yw_s[:, pl.ds(at[u], PAIR)] = jnp.dot(vt, both, preferred_element_type=F32)
            zero = jnp.zeros_like(vt)
            split = jnp.concatenate([jnp.where(left, vt, zero), jnp.where(left, zero, vt)], axis=0)
            updates.append(jnp.dot(split, work[u][2], preferred_element_type=F32))
        for u in range(U1):
            d0, d1 = work[u][3], work[u][4]
            middle = d0 * state + updates[u][0:BLOCK, :]
            pre_s[pl.ds(at[u], BLOCK), :] = state
            pre_s[pl.ds(pl.multiple_of(at[u] + BLOCK, BLOCK), BLOCK), :] = middle
            half = decay * d0
            dec_s[pl.ds(pl.multiple_of((i * U1 + u) * 8, 8), 8), :] = jnp.concatenate(
                [decay, half, jnp.zeros((6, KEY_DIM), F32)], axis=0
            )
            state = d1 * middle + updates[u][BLOCK:PAIR, :]
            decay = half * d1
        return state, decay

    state, decay = lax.fori_loop(
        0, TOK // (PAIR * U1), local_pairs,
        (jnp.zeros((VAL_DIM, KEY_DIM), F32), jnp.ones((1, KEY_DIM), F32)),
    )
    decay_hi = decay.astype(BF16).astype(F32)
    row16 = lax.broadcasted_iota(jnp.int32, (16, KEY_DIM), 0)
    tail = jnp.where(row16 == 0, decay_hi, jnp.where(row16 == 1, decay - decay_hi, 0.0))
    cs_s[0:VAL_DIM, :] = state.astype(BF16)
    cs_s[VAL_DIM : VAL_DIM + 16, :] = tail.astype(BF16)
    cr_s[me] = jnp.zeros((VAL_DIM + 16, KEY_DIM), BF16)

    def hand_on(k):
        return remote(cs_s, cr_s.at[me], csend.at[k], crecv.at[me], moved(me, offs[k], E), t)

    def handed(k):
        source = moved(me, offs[k], E, back=True)
        return remote(cs_s, cr_s.at[source], csend.at[k], crecv.at[source], source, t)

    pl.semaphore_wait(barrier, E - 1 + 3)
    for k in range(1, E):
        hand_on(k).start()

    loads[3].wait()
    loads[4].wait()
    gain_half = fgain_ref[:, pl.ds(pl.multiple_of(c * H, 128), H)]

    def norm_rows(i, carry):
        rows = pl.ds(pl.multiple_of(i * 64, 64), 64)
        a, b = x_s[0, rows, :].astype(F32), x_s[1, rows, :].astype(F32)
        total = jnp.sum(a * a + b * b, axis=-1, keepdims=True)
        factor = lax.rsqrt(total / D + EPS)
        n_s[rows, :] = (x_s[c, rows, :].astype(F32) * factor * gain_half).astype(BF16)
        return carry

    lax.fori_loop(0, NTOK // 64, norm_rows, 0)

    for g in range(NG):
        fill_group(g)
    r_s[c, :, 0:KR, :] = s_s[:, 0:KR, :]
    for k in range(1, E):
        handed(k).wait_recv()
    for k in range(1, E):
        dispatch(0, k).start()

    start = jnp.zeros((VAL_DIM, KEY_DIM), F32)
    for j in range(E - 1):
        ends = cr_s[j, VAL_DIM : VAL_DIM + 16, :].astype(F32)
        after = (ends[0:1, :] + ends[1:2, :]) * start + cr_s[j, 0:VAL_DIM, :].astype(F32)
        start = jnp.where(j < me, after, start)
    ga = lax.broadcasted_iota(jnp.int32, (VAL_DIM, VAL_DIM), 0)
    gb = lax.broadcasted_iota(jnp.int32, (VAL_DIM, VAL_DIM), 1)
    head_gain = jnp.sum(jnp.where(ga == gb, hgain_ref[...], 0.0), axis=-1, keepdims=True)
    own_rows = pl.multiple_of(t * VAL_DIM, VAL_DIM)

    loads[5].wait()

    def finish_pairs(i, carry):
        left = lax.broadcasted_iota(jnp.int32, (BLOCK, PAIR), 1) < BLOCK
        at = [pl.multiple_of((i * U1 + u) * PAIR, PAIR) for u in range(U1)]
        across = []
        for u in range(U1):
            d = dec_s[pl.ds(pl.multiple_of((i * U1 + u) * 8, 8), 8), :]
            s0 = pre_s[pl.ds(at[u], BLOCK), :] + d[0:1, :] * start
            s1 = pre_s[pl.ds(pl.multiple_of(at[u] + BLOCK, BLOCK), BLOCK), :] + d[1:2, :] * start
            states = jnp.concatenate([s0, s1], axis=0).astype(BF16)
            across.append(
                lax.dot_general(states, qe_s[pl.ds(at[u], PAIR), :], NT, preferred_element_type=F32)
            )
        for u in range(U1):
            cols = pl.ds(at[u], PAIR)
            y = yw_s[:, cols] + jnp.where(left, across[u][0:BLOCK, :], across[u][BLOCK:PAIR, :])
            factor = lax.rsqrt(jnp.mean(y * y, axis=0, keepdims=True) + EPS)
            gate = o_s[:, cols].astype(F32)
            gate = gate * (1.0 / (1.0 + jnp.exp(-gate)))
            m_s[pl.ds(own_rows, VAL_DIM), cols] = (y * factor * head_gain * gate).astype(BF16)
        return carry

    lax.fori_loop(0, TOK // (PAIR * U1), finish_pairs, 0)

    VH = VAL_DIM // 2
    reach = {(1, 0): Z // 2, (1, 1): Z - 1 - Z // 2, (-1, 0): Z - 1 - Z // 2, (-1, 1): Z // 2}

    def head_at(zz, core):
        return pl.multiple_of((lax.rem(zz + 2 * Z, Z) * 2 + core) * VAL_DIM, VAL_DIM)

    def ring(way, half, hop):
        rows = pl.ds(pl.multiple_of(head_at(z - way * (hop - 1), c) + half * VH, VH), VH)
        w = 0 if way == 1 else 1
        return remote(
            m_s.at[rows, :], m_s.at[rows, :], msend.at[w, half, hop - 1], mrecv.at[w, half, hop - 1],
            me, lax.rem(z + way + Z, Z) * 2 + c,
        )

    def ringed(way, half, hop):
        rows = pl.ds(pl.multiple_of(head_at(z - way * hop, c) + half * VH, VH), VH)
        w = 0 if way == 1 else 1
        return remote(
            m_s.at[rows, :], m_s.at[rows, :], msend.at[w, half, hop - 1], mrecv.at[w, half, hop - 1],
            me, lax.rem(z + way + Z, Z) * 2 + c,
        )

    def share(r, core):
        rows = pl.ds(head_at(z - r, core), VAL_DIM)
        return remote(m_s.at[rows, :], m_s.at[rows, :], dsend.at[r], drecv.at[r], me, z * 2 + pc)

    lanes = [(1, 0), (-1, 1), (1, 1), (-1, 0)]

    def relay(hop):
        for way, half in lanes:
            if hop <= reach[way, half]:
                ringed(way, half, hop).wait_recv()
                if hop + 1 <= reach[way, half]:
                    ring(way, half, hop + 1).start()
        if hop == Z - hop:
            share(hop, c).start()
        elif hop < Z - hop:
            share(hop, c).start()
            share(Z - hop, c).start()

    for way, half in lanes:
        if reach[way, half] >= 1:
            ring(way, half, 1).start()
    share(0, c).start()

    def swapper(ref, outer, inner):
        size = outer * inner * UNIT
        row = lax.broadcasted_iota(jnp.int32, (size, 1), 0)
        source = (row // UNIT % inner * outer + row // (inner * UNIT)) * UNIT + row % UNIT
        ref[...] = jnp.where(lax.broadcasted_iota(jnp.int32, (size, size), 1) == source, 1.0, 0.0).astype(BF16)

    swapper(perm_s, Z, SG)
    swapper(perm_back_s, SG, J)

    def forward_group(w, g):
        for k in range(g * KG, (g + 1) * KG):
            if k:
                dispatch(w, k).wait_recv()
        forward(w, g, c).start()

    def ffn(w, g):
        rows = slice(g * GR, (g + 1) * GR)
        forward(w, g, pc).wait_recv()
        a, b = r_s[0, w, rows, :], r_s[1, w, rows, :]
        ca, cb = slice(w * HW, (w + 1) * HW), slice(H + w * HW, H + (w + 1) * HW)

        def product(weight):
            return lax.dot_general(a, weight[:, ca], NT, preferred_element_type=F32) + lax.dot_general(
                b, weight[:, cb], NT, preferred_element_type=F32
            )

        gate, up = product(wg_s), product(wu_s)
        if w:
            gate, up = gate + ga_s[rows, :], up + ua_s[rows, :]
        if w < NW - 1:
            ga_s[rows, :] = gate
            ua_s[rows, :] = up
        else:
            hid_s[rows, :] = (gate * (1.0 / (1.0 + jnp.exp(-gate))) * up).astype(BF16)

    def relative(r):
        return lax.rem(z + r + 2 * Z, Z)

    def swap(g, r):
        part = relative(r)
        return remote(
            pp_s.at[pc, :, g, part], qb_s.at[:, g, part], psend.at[g, r % Z], precv.at[g, r % Z],
            me, z * 2 + pc,
        )

    def way_of(d):
        return 1 - 2 * (d % 2)

    def pass_on(g, d, s):
        way = way_of(d)
        part = relative(-way * (1 + s))
        return remote(
            pp_s.at[c, d, g, part], rb_s.at[s, g, d], bsend.at[s, g, d], brecv.at[s, g, d],
            me, relative(way) * 2 + c,
        )

    swapped = set()

    def add_and_pass(g, d, s):
        r = -way_of(d) * (1 + s)
        part = relative(r)
        if (g, r % Z) not in swapped:
            swapped.add((g, r % Z))
            swap(g, r).wait_recv()
        total = pp_s[c, d, g, part].astype(F32) + qb_s[d, g, part].astype(F32)
        if s:
            pass_on(g, d, s - 1).wait_recv()
            total = total + rb_s[s - 1, g, d].astype(F32)
        if s < Z - 1:
            pp_s[c, d, g, part] = total.astype(BF16)
            pass_on(g, d, s).start()
        else:
            for n in range(W // 128):
                at = (d * (W // 128) + n) * SR
                fs_s[g, at : at + SR, :] = total[:, n * 128 : n * 128 + 128].astype(BF16)

    def down(g):
        rows = slice(g * Z * SR, (g + 1) * Z * SR)
        hp_s[rows, :] = jnp.dot(
            perm_s[...], hid_s[rows, :], preferred_element_type=F32
        ).astype(BF16)
        turns = [r for n in range(1, Z // 2) for r in (-n, n)] + [Z // 2, 0]
        for n in range(0, Z, 2):
            pair = turns[n : n + 2]
            hid = jnp.concatenate(
                [
                    hp_s[pl.ds(pl.multiple_of((g * Z + relative(r)) * SR, 16), SR), :]
                    for r in pair
                ],
                axis=0,
            )
            for half in range(2):
                for d in range(ND):
                    cols = slice(half * H + d * W, half * H + (d + 1) * W)
                    y = jnp.dot(hid, wd_s[:, cols], preferred_element_type=F32).astype(BF16)
                    for i, r in enumerate(pair):
                        pp_s[half, d, g, relative(r)] = y[i * SR : (i + 1) * SR, :]
            for r in pair:
                swap(g, r).start()
            if n == min(2, Z - 2):
                for d in range(ND):
                    add_and_pass(g, d, 0)

    hops = max(reach.values())
    for load in loads[6:]:
        load.wait()
    half = NG // 2
    todo = list(range(1, hops + 1))

    def next_hop():
        if todo:
            relay(todo.pop(0))

    next_hop()
    for w in range(1, NW):
        for k in range(1, E):
            dispatch(w, k).start()
        for g in range(NG):
            forward_group(w - 1, g)
        next_hop()
        for g in range(NG):
            ffn(w - 1, g)
    while todo:
        next_hop()
    forward_group(NW - 1, 0)
    for g in range(half):
        forward_group(NW - 1, g + 1)
        ffn(NW - 1, g)
    down(0)
    for g in range(half, NG):
        if g + 1 < NG:
            forward_group(NW - 1, g + 1)
        ffn(NW - 1, g)
    ahead = 1 if Z > 2 else 0
    if ahead:
        for d in range(ND):
            add_and_pass(0, d, ahead)
    if NS > 1:
        down(1)

    out_copy = pltpu.make_async_copy(out_s, out_hbm, osem)

    def project(n):
        for r in range(Z) if n == 0 else ():
            share(r, pc).wait_recv()
        cols = slice(n * (TOK // 4), (n + 1) * (TOK // 4))
        outt = lax.dot_general(
            wo_s[...], m_s[:, cols], (((0,), (0,)), ((), ())), preferred_element_type=F32
        )
        out_s[cols, :] = outt.T.astype(BF16)
        if n == 3:
            out_copy.start()

    lanes_out = J * 2 * SUB
    lane = lax.broadcasted_iota(jnp.int32, (1, lanes_out), 1)

    def weigh_all():
        token = lax.broadcasted_iota(jnp.int32, (NTOK, lanes_out), 0)
        mine = z * 2 * SUB + lane % (2 * SUB)
        pick = jnp.where(token == mine, 1.0, 0.0).astype(BF16)
        local = slot_s[...] - (z * UNIT).astype(F32)
        local = jnp.where((local >= 0) & (local < UNIT), local, -1.0).astype(BF16)
        place_at = jnp.dot(local, pick, preferred_element_type=F32)
        high = jnp.dot(weight_hi, pick, preferred_element_type=F32)
        low = jnp.dot(weight_lo, pick, preferred_element_type=F32)
        shift = (lane // (2 * SUB) * UNIT).astype(F32)
        target = jnp.where(place_at >= 0, place_at + shift, -1.0)
        row = lax.broadcasted_iota(jnp.int32, (J * UNIT, lanes_out), 0).astype(F32)
        for k in range(E):
            rows = slice(k * J * UNIT, (k + 1) * J * UNIT)
            here = row == target[k : k + 1, :]
            gh_s[rows, :] = jnp.where(here, high[k : k + 1, :], 0.0).astype(BF16)
            gl_s[rows, :] = jnp.where(here, low[k : k + 1, :], 0.0).astype(BF16)

    BR = J * UNIT

    def give_back(k):
        rows = slice(k * BR, (k + 1) * BR)
        return remote(
            fb_s.at[rows, :], rr_s.at[rows, :], rsend.at[k], rrecv.at[k], moved(me, offs[k], E, back=True), t
        )

    side = [functools.partial(project, n) for n in range(4)] + [weigh_all]
    def last(g):
        rows = slice(g * SG * BR, (g + 1) * SG * BR)
        fb_s[rows, :] = jnp.dot(perm_back_s[...], fs_s[g], preferred_element_type=F32).astype(BF16)
        for k in range(g * SG, (g + 1) * SG):
            if k:
                give_back(k).start()

    for s in range(1, Z):
        for g in reversed(range(NS)):
            step = s if g else s + ahead
            if step < Z:
                for d in range(ND):
                    add_and_pass(g, d, step)
            if step == Z - 1:
                last(g)
        if s < Z - 1:
            for _ in range(-(-len(side) // max(1, Z - 1 - s))):
                side.pop(0)()
    while side:
        side.pop(0)()
    rr_s[0:BR, :] = fb_s[0:BR, :]
    for k in range(1, E):
        give_back(k).wait_recv()
    results = rr_s[...].T
    combined = jnp.dot(results, gh_s[...], preferred_element_type=F32) + jnp.dot(
        results, gl_s[...], preferred_element_type=F32
    )
    combined = combined.T.astype(BF16)
    for j in range(J):
        co_s[j] = combined[j * 2 * SUB : (j + 1) * 2 * SUB, :]

    def hand_over(core):
        mine = pl.ds(pl.multiple_of((1 - core) * SUB, SUB), SUB)
        return remote(co_s.at[:, mine, :], mo_s.at[core], zsend, zrecv, me, z * 2 + pc)

    hand_over(c).start()
    mo_s[c] = co_s[:, pl.ds(pl.multiple_of(c * SUB, SUB), SUB), :]
    hand_over(pc).wait_recv()
    for half in range(2):
        for j in range(J):
            moe_ref[:, half * H + j * 128 : half * H + (j + 1) * 128] = mo_s[half, j]

    for k in range(1, E):
        for w in range(NW):
            dispatch(w, k).wait_send()
        hand_on(k).wait_send()
        give_back(k).wait_send()
    for w in range(NW):
        for g in range(NG):
            forward(w, g, c).wait_send()
    for way, half in lanes:
        for hop in range(1, reach[way, half] + 1):
            ring(way, half, hop).wait_send()
    for r in range(Z):
        share(r, c).wait_send()
    for g in range(NS):
        for r in range(Z):
            swap(g, r).wait_send()
        for d in range(ND):
            for s in range(Z - 1):
                pass_on(g, d, s).wait_send()
    hand_over(c).wait_send()
    out_copy.wait()


def on_device(
    query, forget, values, out_gate, gap, extra, head_gain, w_out,
    tokens, ff_gain, chosen, chosen_w, w_gate, w_up, w_down,
):
    E, TP = w_gate.shape[0] * lax.axis_size("ep"), lax.axis_size("tp")
    TOK, D = query.shape[0], tokens.shape[1]
    NTOK, FF = tokens.shape[0], w_gate.shape[2]
    SUB = NTOK // TP
    CAP = max(2, SUB * TOPK * 5 // (4 * E))
    Z, KR = TP // 2, TP * CAP
    ROWS, H = E * KR, D // 2
    KG = max(1, E // 4)
    NG = E // KG
    SG = max(1, E // 2)
    NS, UNIT, J = E // SG, 2 * CAP, H // 128
    SR = SG * UNIT
    ND = 4 if H % 512 == 0 else 2
    NW = 2
    cfg = dict(E=E, TP=TP, TOK=TOK, SUB=SUB, CAP=CAP, ND=ND, NW=NW)
    any_spec = pl.BlockSpec(memory_space=pl.ANY)
    hbm = pl.BlockSpec(memory_space=pl.ANY)
    vmem = pl.BlockSpec(memory_space=pltpu.VMEM)
    dma = pltpu.SemaphoreType.DMA
    V = pltpu.VMEM
    hops = Z // 2
    return pl.pallas_call(
        functools.partial(kernel, cfg),
        out_shape=(
            jax.ShapeDtypeStruct((TOK, w_out.shape[1]), BF16),
            jax.ShapeDtypeStruct((SUB, D), BF16),
        ),
        in_specs=[hbm] * 4 + [vmem] * 3 + [hbm] * 2 + [vmem] * 3 + [hbm] * 3,
        out_specs=(any_spec, vmem),
        scratch_shapes=[
            V((TOK, KEY_DIM), BF16), V((TOK, KEY_DIM), BF16), V((VAL_DIM, TOK), BF16), V((VAL_DIM, TOK), BF16),
            V(w_out.shape, BF16), V((2, NTOK, H), BF16), V((FF, D), BF16), V((FF, D), BF16), V((FF, D), BF16),
            V((PAIR, PAIR), F32), V((TOK // PAIR * 8, KEY_DIM), F32), V((TOK, KEY_DIM), F32),
            V((VAL_DIM, TOK), F32), V((TOK, KEY_DIM), BF16), V((VAL_DIM + 16, KEY_DIM), BF16),
            V((E, VAL_DIM + 16, KEY_DIM), BF16),
            V((NTOK, H), BF16), V((E, NTOK), F32), V((ROWS, NTOK), BF16), V((NW, ROWS, H // NW), BF16),
            V((2, NW, ROWS, H // NW), BF16), V((ROWS, FF), F32), V((ROWS, FF), F32),
            V((ROWS, FF), BF16), V((ROWS, FF), BF16),
            V((2, ND, NS, Z, SR, H // ND), BF16), V((ND, NS, Z, SR, H // ND), BF16),
            V((Z - 1, NS, ND, SR, H // ND), BF16),
            V((Z * SR, Z * SR), BF16), V((J * SR, J * SR), BF16),
            V((TP * VAL_DIM, TOK), BF16), V((TOK, w_out.shape[1]), BF16), V((NS, J * SR, 128), BF16),
            V((E * J * UNIT, 128), BF16), V((E * J * UNIT, 128), BF16),
            V((E * J * UNIT, J * 2 * SUB), BF16), V((E * J * UNIT, J * 2 * SUB), BF16),
            V((J, 2 * SUB, 128), BF16), V((2, J, SUB, 128), BF16),
            dma((10,)), dma, dma((NW, E)), dma((NW, E)), dma((NW, NG)), dma((NW, NG)), dma((E,)), dma((E,)),
            dma((2, 2, hops)), dma((2, 2, hops)), dma((Z,)), dma((Z,)), dma((NS, Z)), dma((NS, Z)),
            dma((Z - 1, NS, ND)), dma((Z - 1, NS, ND)), dma((E,)), dma((E,)), dma, dma,
        ],
        compiler_params=pltpu.CompilerParams(
            collective_id=0, has_side_effects=True, vmem_limit_bytes=64000 * 1024
        ),
    )(
        query, forget, values.T, out_gate.T, gap.reshape(1, -1), extra.T, head_gain.reshape(1, -1), w_out,
        tokens, ff_gain.reshape(1, -1), chosen.T, chosen_w.T, w_gate[0].T, w_up[0].T, w_down[0],
    )


def solution(mesh):
    placed = (
        P("ep", "tp"), P("ep", "tp"), P("ep", "tp"), P("ep", "tp"), P("tp"), P("ep", "tp"), P("tp"),
        P(None, "tp"), P("ep", None), P(), P("ep", None), P("ep", None),
        P("ep", None, "tp"), P("ep", None, "tp"), P("ep", "tp", None),
    )
    return jax.shard_map(
        on_device,
        mesh=mesh,
        in_specs=placed,
        out_specs=(P("ep", "tp"), P(("ep", "tp"), None)),
        check_vma=False,
    )
```

```python
import functools

import jax
import jax.numpy as jnp
from jax import lax
from jax.experimental import pallas as pl
from jax.experimental.pallas import tpu as pltpu
from jax.sharding import PartitionSpec as P

KEY_DIM = 128
VAL_DIM = 64
BLOCK = 64
PAIR = 128
TOPK = 2
EPS = 1e-06
MESH = pl.DeviceIdType.MESH
F32 = jnp.float32
BF16 = jnp.bfloat16
NT = (((1,), (1,)), ((), ()))


def offsets(experts):
    if experts == 16:
        return [
            (0, 0), (2, 2), (1, 2), (2, 1),
            (3, 2), (2, 3), (0, 1), (3, 0),
            (1, 1), (3, 3), (0, 2), (2, 0),
            (1, 3), (3, 1), (0, 3), (1, 0),
        ]
    return [(0, k) for k in range(experts)]


def moved(me, step, experts, back=False):
    dy, dx = step
    if experts != 16:
        return lax.rem(me + (experts - dx if back else dx), experts)
    y, x = me // 4, lax.rem(me, 4)
    if back:
        dy, dx = (4 - dy) % 4, (4 - dx) % 4
    return lax.rem(y + dy, 4) * 4 + lax.rem(x + dx, 4)


def kernel(
    cfg,
    q_hbm, f_hbm, v_hbm, o_hbm, gap_ref, extra_ref, hgain_ref, wo_hbm,
    x_hbm, fgain_ref, idx_ref, wt_ref, wg_hbm, wu_hbm, wd_hbm,
    out_hbm, moe_ref,
    q_s, f_s, v_s, o_s, wo_s, x_s, wg_s, wu_s, wd_s,
    tri_s, dec_s, pre_s, yw_s, qe_s, cs_s, cr_s,
    n_s, slot_s, g_s, s_s, r_s, ga_s, ua_s, hid_s, hp_s, pp_s, qb_s, rb_s,
    perm_s, perm_back_s, m_s, out_s, fs_s, fb_s, rr_s, gh_s, gl_s, co_s, mo_s,
    lsem, osem, asend, arecv, fsend, frecv, csend, crecv,
    msend, mrecv, dsend, drecv, psend, precv, bsend, brecv, rsend, rrecv, zsend, zrecv,
):
    E, TP, TOK, SUB, CAP = cfg["E"], cfg["TP"], cfg["TOK"], cfg["SUB"], cfg["CAP"]
    Z = TP // 2
    KR = TP * CAP
    KG = max(1, E // 4)
    NG = E // KG
    GR = KG * KR
    UNIT = 2 * CAP
    SG = max(1, E // 2)
    NS = E // SG
    SR = SG * UNIT
    D = x_hbm.shape[1]
    H = D // 2
    ND = cfg["ND"]
    W = H // ND
    NW = cfg["NW"]
    HW = H // NW
    J = H // 128
    NTOK = x_hbm.shape[0]
    offs = offsets(E)
    me = lax.axis_index("ep")
    t = lax.axis_index("tp")
    z, c = t // 2, lax.rem(t, 2)
    pc = 1 - c

    def remote(src, dst, ss, rs, e, tt):
        return pltpu.make_async_remote_copy(
            src_ref=src, dst_ref=dst, send_sem=ss, recv_sem=rs, device_id=(e, tt), device_id_type=MESH
        )

    loads = [
        (f_hbm, f_s), (q_hbm, q_s), (v_hbm, v_s), (x_hbm.at[:, 0:H], x_s.at[0]), (x_hbm.at[:, H:D], x_s.at[1]),
        (o_hbm, o_s),
        (wg_hbm, wg_s), (wu_hbm, wu_s), (wd_hbm, wd_s), (wo_hbm, wo_s),
    ]
    loads = [pltpu.make_async_copy(a, b, lsem.at[i]) for i, (a, b) in enumerate(loads)]
    for load in loads:
        load.start()
    barrier = pltpu.get_barrier_semaphore()
    for k in range(1, E):
        pl.semaphore_signal(barrier, inc=1, device_id=(moved(me, offs[k], E), t), device_id_type=MESH)
    for j in (z * 2 + pc, lax.rem(z + 1, Z) * 2 + c, lax.rem(z + Z - 1, Z) * 2 + c):
        pl.semaphore_signal(barrier, inc=1, device_id=(me, j), device_id_type=MESH)

    i0, i1 = idx_ref[0:1, :], idx_ref[1:2, :]
    row_e = lax.broadcasted_iota(jnp.int32, (E, NTOK), 0)
    expert_of = jnp.zeros((E, NTOK), jnp.int32)
    for k in range(E):
        expert_of = jnp.where(row_e == k, moved(me, offs[k], E), expert_of)
    first, second = expert_of == i0, expert_of == i1
    chosen = jnp.where(first | second, 1.0, 0.0)
    ra = lax.broadcasted_iota(jnp.int32, (NTOK, NTOK), 0)
    rb = lax.broadcasted_iota(jnp.int32, (NTOK, NTOK), 1)
    before = jnp.where((ra // SUB == rb // SUB) & (ra < rb), 1.0, 0.0).astype(BF16)
    place = jnp.dot(chosen.astype(BF16), before, preferred_element_type=F32)
    block_of = (lax.broadcasted_iota(jnp.int32, (E, NTOK), 1) // SUB).astype(F32)
    slot_s[...] = jnp.where(chosen > 0, CAP * block_of + place, -1.0)
    weight = jnp.where(first, wt_ref[0:1, :], 0.0) + jnp.where(second, wt_ref[1:2, :], 0.0)
    weight_hi = weight.astype(BF16)
    weight_lo = (weight - weight_hi.astype(F32)).astype(BF16)

    place_row = lax.broadcasted_iota(jnp.int32, (KR, NTOK), 0).astype(F32)

    def fill_group(g):
        for k in range(g * KG, (g + 1) * KG):
            rows = slice(k * KR, (k + 1) * KR)
            g_s[rows, :] = jnp.where(place_row == slot_s[k : k + 1, :], 1.0, 0.0).astype(BF16)
        rows = slice(g * GR, (g + 1) * GR)
        pick = g_s[rows, :]
        for n in range(0, H, min(HW, 256)):
            at = n % HW
            s_s[n // HW, rows, at : at + min(HW, 256)] = jnp.dot(
                pick, n_s[:, n : n + min(HW, 256)], preferred_element_type=F32
            ).astype(BF16)

    def dispatch(w, k):
        rows = slice(k * KR, (k + 1) * KR)
        return remote(
            s_s.at[w, rows, :], r_s.at[c, w, rows, :], asend.at[w, k], arecv.at[w, k],
            moved(me, offs[k], E), t,
        )

    def forward(w, g, core):
        rows = slice(g * GR, (g + 1) * GR)
        return remote(
            r_s.at[core, w, rows, :], r_s.at[core, w, rows, :], fsend.at[w, g], frecv.at[w, g], me, z * 2 + pc
        )

    ta = lax.broadcasted_iota(jnp.int32, (PAIR, PAIR), 0)
    tb = lax.broadcasted_iota(jnp.int32, (PAIR, PAIR), 1)
    tri = (ta // BLOCK == tb // BLOCK) & (ta >= tb)
    tri_s[...] = jnp.where(tri, 1.0, 0.0)
    gap = gap_ref[...]
    for load in loads[0:3]:
        load.wait()
    U1 = min(4, TOK // PAIR)

    def local_pairs(i, carry):
        state, decay = carry
        trif = tri_s[...]
        trib = trif.astype(BF16)
        in_first = lax.broadcasted_iota(jnp.int32, (PAIR, PAIR), 0) < BLOCK
        left = lax.broadcasted_iota(jnp.int32, (BLOCK, PAIR), 1) < BLOCK
        later = lax.broadcasted_iota(jnp.int32, (PAIR, PAIR), 1)
        earlier = lax.broadcasted_iota(jnp.int32, (PAIR, PAIR), 0)
        maskt = (later // BLOCK == earlier // BLOCK) & (earlier <= later)
        at = [pl.multiple_of((i * U1 + u) * PAIR, PAIR) for u in range(U1)]
        keys, cums = [], []
        for u in range(U1):
            gate = f_s[pl.ds(at[u], PAIR), :].astype(F32)
            key = gap * (1.0 / (1.0 + jnp.exp(gate)))
            logf = jnp.log(1.0 - key)
            hi = logf.astype(BF16)
            lo = (logf - hi.astype(F32)).astype(BF16)
            cum = jnp.dot(trib, hi, preferred_element_type=F32) + jnp.dot(
                trib, lo, preferred_element_type=F32
            )
            extra = jnp.sum(trif * extra_ref[:, pl.ds(at[u], PAIR)], axis=-1, keepdims=True)
            keys.append(key)
            cums.append(cum + extra)
        work = []
        for u in range(U1):
            key, cum = keys[u], cums[u]
            mid0, mid1 = cum[31:32, :], cum[95:96, :]
            end0, end1 = cum[63:64, :], cum[127:128, :]
            away = cum - jnp.where(in_first, mid0, mid1)
            query = q_s[pl.ds(at[u], PAIR), :].astype(F32)
            query = query * (1.0 / (1.0 + jnp.exp(-query)))
            qs = query * jnp.exp(away)
            ks = key * jnp.exp(-away)
            qe = qs * jnp.where(in_first, jnp.exp(mid0), jnp.exp(mid1))
            ke = ks * jnp.where(in_first, jnp.exp(end0 - mid0), jnp.exp(end1 - mid1))
            qe_s[pl.ds(at[u], PAIR), :] = qe.astype(BF16)
            work.append((qs.astype(BF16), ks.astype(BF16), ke.astype(BF16), jnp.exp(end0), jnp.exp(end1)))
        scores = [lax.dot_general(w[1], w[0], NT, preferred_element_type=F32) for w in work]
        updates = []
        for u in range(U1):
            vt = v_s[:, pl.ds(at[u], PAIR)]
            both = jnp.where(maskt, scores[u], 0.0).astype(BF16)
            yw_s[:, pl.ds(at[u], PAIR)] = jnp.dot(vt, both, preferred_element_type=F32)
            zero = jnp.zeros_like(vt)
            split = jnp.concatenate([jnp.where(left, vt, zero), jnp.where(left, zero, vt)], axis=0)
            updates.append(jnp.dot(split, work[u][2], preferred_element_type=F32))
        for u in range(U1):
            d0, d1 = work[u][3], work[u][4]
            middle = d0 * state + updates[u][0:BLOCK, :]
            pre_s[pl.ds(at[u], BLOCK), :] = state
            pre_s[pl.ds(pl.multiple_of(at[u] + BLOCK, BLOCK), BLOCK), :] = middle
            half = decay * d0
            dec_s[pl.ds(pl.multiple_of((i * U1 + u) * 8, 8), 8), :] = jnp.concatenate(
                [decay, half, jnp.zeros((6, KEY_DIM), F32)], axis=0
            )
            state = d1 * middle + updates[u][BLOCK:PAIR, :]
            decay = half * d1
        return state, decay

    state, decay = lax.fori_loop(
        0, TOK // (PAIR * U1), local_pairs,
        (jnp.zeros((VAL_DIM, KEY_DIM), F32), jnp.ones((1, KEY_DIM), F32)),
    )
    decay_hi = decay.astype(BF16).astype(F32)
    row16 = lax.broadcasted_iota(jnp.int32, (16, KEY_DIM), 0)
    tail = jnp.where(row16 == 0, decay_hi, jnp.where(row16 == 1, decay - decay_hi, 0.0))
    cs_s[0:VAL_DIM, :] = state.astype(BF16)
    cs_s[VAL_DIM : VAL_DIM + 16, :] = tail.astype(BF16)
    cr_s[me] = jnp.zeros((VAL_DIM + 16, KEY_DIM), BF16)

    def hand_on(k):
        return remote(cs_s, cr_s.at[me], csend.at[k], crecv.at[me], moved(me, offs[k], E), t)

    def handed(k):
        source = moved(me, offs[k], E, back=True)
        return remote(cs_s, cr_s.at[source], csend.at[k], crecv.at[source], source, t)

    pl.semaphore_wait(barrier, E - 1 + 3)
    for k in range(1, E):
        hand_on(k).start()

    loads[3].wait()
    loads[4].wait()
    gain_half = fgain_ref[:, pl.ds(pl.multiple_of(c * H, 128), H)]

    def norm_rows(i, carry):
        rows = pl.ds(pl.multiple_of(i * 64, 64), 64)
        a, b = x_s[0, rows, :].astype(F32), x_s[1, rows, :].astype(F32)
        total = jnp.sum(a * a + b * b, axis=-1, keepdims=True)
        factor = lax.rsqrt(total / D + EPS)
        n_s[rows, :] = (x_s[c, rows, :].astype(F32) * factor * gain_half).astype(BF16)
        return carry

    lax.fori_loop(0, NTOK // 64, norm_rows, 0)

    for g in range(NG):
        fill_group(g)
    r_s[c, :, 0:KR, :] = s_s[:, 0:KR, :]
    for k in range(1, E):
        handed(k).wait_recv()
    for k in range(1, E):
        dispatch(0, k).start()

    start = jnp.zeros((VAL_DIM, KEY_DIM), F32)
    for j in range(E - 1):
        ends = cr_s[j, VAL_DIM : VAL_DIM + 16, :].astype(F32)
        after = (ends[0:1, :] + ends[1:2, :]) * start + cr_s[j, 0:VAL_DIM, :].astype(F32)
        start = jnp.where(j < me, after, start)
    ga = lax.broadcasted_iota(jnp.int32, (VAL_DIM, VAL_DIM), 0)
    gb = lax.broadcasted_iota(jnp.int32, (VAL_DIM, VAL_DIM), 1)
    head_gain = jnp.sum(jnp.where(ga == gb, hgain_ref[...], 0.0), axis=-1, keepdims=True)
    own_rows = pl.multiple_of(t * VAL_DIM, VAL_DIM)

    loads[5].wait()

    def finish_pairs(i, carry):
        left = lax.broadcasted_iota(jnp.int32, (BLOCK, PAIR), 1) < BLOCK
        at = [pl.multiple_of((i * U1 + u) * PAIR, PAIR) for u in range(U1)]
        across = []
        for u in range(U1):
            d = dec_s[pl.ds(pl.multiple_of((i * U1 + u) * 8, 8), 8), :]
            s0 = pre_s[pl.ds(at[u], BLOCK), :] + d[0:1, :] * start
            s1 = pre_s[pl.ds(pl.multiple_of(at[u] + BLOCK, BLOCK), BLOCK), :] + d[1:2, :] * start
            states = jnp.concatenate([s0, s1], axis=0).astype(BF16)
            across.append(
                lax.dot_general(states, qe_s[pl.ds(at[u], PAIR), :], NT, preferred_element_type=F32)
            )
        for u in range(U1):
            cols = pl.ds(at[u], PAIR)
            y = yw_s[:, cols] + jnp.where(left, across[u][0:BLOCK, :], across[u][BLOCK:PAIR, :])
            factor = lax.rsqrt(jnp.mean(y * y, axis=0, keepdims=True) + EPS)
            gate = o_s[:, cols].astype(F32)
            gate = gate * (1.0 / (1.0 + jnp.exp(-gate)))
            m_s[pl.ds(own_rows, VAL_DIM), cols] = (y * factor * head_gain * gate).astype(BF16)
        return carry

    lax.fori_loop(0, TOK // (PAIR * U1), finish_pairs, 0)

    VH = VAL_DIM // 2
    reach = {(1, 0): Z // 2, (1, 1): Z - 1 - Z // 2, (-1, 0): Z - 1 - Z // 2, (-1, 1): Z // 2}

    def head_at(zz, core):
        return pl.multiple_of((lax.rem(zz + 2 * Z, Z) * 2 + core) * VAL_DIM, VAL_DIM)

    def ring(way, half, hop):
        rows = pl.ds(pl.multiple_of(head_at(z - way * (hop - 1), c) + half * VH, VH), VH)
        w = 0 if way == 1 else 1
        return remote(
            m_s.at[rows, :], m_s.at[rows, :], msend.at[w, half, hop - 1], mrecv.at[w, half, hop - 1],
            me, lax.rem(z + way + Z, Z) * 2 + c,
        )

    def ringed(way, half, hop):
        rows = pl.ds(pl.multiple_of(head_at(z - way * hop, c) + half * VH, VH), VH)
        w = 0 if way == 1 else 1
        return remote(
            m_s.at[rows, :], m_s.at[rows, :], msend.at[w, half, hop - 1], mrecv.at[w, half, hop - 1],
            me, lax.rem(z + way + Z, Z) * 2 + c,
        )

    def share(r, core):
        rows = pl.ds(head_at(z - r, core), VAL_DIM)
        return remote(m_s.at[rows, :], m_s.at[rows, :], dsend.at[r], drecv.at[r], me, z * 2 + pc)

    lanes = [(1, 0), (-1, 1), (1, 1), (-1, 0)]

    def relay(hop):
        for way, half in lanes:
            if hop <= reach[way, half]:
                ringed(way, half, hop).wait_recv()
                if hop + 1 <= reach[way, half]:
                    ring(way, half, hop + 1).start()
        if hop == Z - hop:
            share(hop, c).start()
        elif hop < Z - hop:
            share(hop, c).start()
            share(Z - hop, c).start()

    for way, half in lanes:
        if reach[way, half] >= 1:
            ring(way, half, 1).start()
    share(0, c).start()

    def swapper(ref, outer, inner):
        size = outer * inner * UNIT
        row = lax.broadcasted_iota(jnp.int32, (size, 1), 0)
        source = (row // UNIT % inner * outer + row // (inner * UNIT)) * UNIT + row % UNIT
        ref[...] = jnp.where(lax.broadcasted_iota(jnp.int32, (size, size), 1) == source, 1.0, 0.0).astype(BF16)

    swapper(perm_s, Z, SG)
    swapper(perm_back_s, SG, J)

    def forward_group(w, g):
        for k in range(g * KG, (g + 1) * KG):
            if k:
                dispatch(w, k).wait_recv()
        forward(w, g, c).start()

    def ffn(w, g):
        rows = slice(g * GR, (g + 1) * GR)
        forward(w, g, pc).wait_recv()
        a, b = r_s[0, w, rows, :], r_s[1, w, rows, :]
        ca, cb = slice(w * HW, (w + 1) * HW), slice(H + w * HW, H + (w + 1) * HW)

        def product(weight):
            return lax.dot_general(a, weight[:, ca], NT, preferred_element_type=F32) + lax.dot_general(
                b, weight[:, cb], NT, preferred_element_type=F32
            )

        gate, up = product(wg_s), product(wu_s)
        if w:
            gate, up = gate + ga_s[rows, :], up + ua_s[rows, :]
        if w < NW - 1:
            ga_s[rows, :] = gate
            ua_s[rows, :] = up
        else:
            hid_s[rows, :] = (gate * (1.0 / (1.0 + jnp.exp(-gate))) * up).astype(BF16)

    def relative(r):
        return lax.rem(z + r + 2 * Z, Z)

    def swap(g, r):
        part = relative(r)
        return remote(
            pp_s.at[pc, :, g, part], qb_s.at[:, g, part], psend.at[g, r % Z], precv.at[g, r % Z],
            me, z * 2 + pc,
        )

    def way_of(d):
        return 1 - 2 * (d % 2)

    def pass_on(g, d, s):
        way = way_of(d)
        part = relative(-way * (1 + s))
        return remote(
            pp_s.at[c, d, g, part], rb_s.at[s, g, d], bsend.at[s, g, d], brecv.at[s, g, d],
            me, relative(way) * 2 + c,
        )

    swapped = set()

    def add_and_pass(g, d, s):
        r = -way_of(d) * (1 + s)
        part = relative(r)
        if (g, r % Z) not in swapped:
            swapped.add((g, r % Z))
            swap(g, r).wait_recv()
        total = pp_s[c, d, g, part].astype(F32) + qb_s[d, g, part].astype(F32)
        if s:
            pass_on(g, d, s - 1).wait_recv()
            total = total + rb_s[s - 1, g, d].astype(F32)
        if s < Z - 1:
            pp_s[c, d, g, part] = total.astype(BF16)
            pass_on(g, d, s).start()
        else:
            for n in range(W // 128):
                at = (d * (W // 128) + n) * SR
                fs_s[g, at : at + SR, :] = total[:, n * 128 : n * 128 + 128].astype(BF16)

    def down(g, between=None):
        rows = slice(g * Z * SR, (g + 1) * Z * SR)
        hp_s[rows, :] = jnp.dot(
            perm_s[...], hid_s[rows, :], preferred_element_type=F32
        ).astype(BF16)
        turns = [r for n in range(1, Z // 2) for r in (-n, n)] + [Z // 2, 0]
        for n in range(0, Z, 2):
            pair = turns[n : n + 2]
            hid = jnp.concatenate(
                [
                    hp_s[pl.ds(pl.multiple_of((g * Z + relative(r)) * SR, 16), SR), :]
                    for r in pair
                ],
                axis=0,
            )
            for half in range(2):
                for d in range(ND):
                    cols = slice(half * H + d * W, half * H + (d + 1) * W)
                    y = jnp.dot(hid, wd_s[:, cols], preferred_element_type=F32).astype(BF16)
                    for i, r in enumerate(pair):
                        pp_s[half, d, g, relative(r)] = y[i * SR : (i + 1) * SR, :]
            for r in pair:
                swap(g, r).start()
            if between and n == 2:
                between()
            if n == min(2, Z - 2):
                for d in range(ND):
                    add_and_pass(g, d, 0)

    hops = max(reach.values())
    for load in loads[6:]:
        load.wait()
    half = NG // 2
    todo = list(range(1, hops + 1))

    def next_hop():
        if todo:
            relay(todo.pop(0))

    next_hop()
    for w in range(1, NW):
        for k in range(1, E):
            dispatch(w, k).start()
        for g in range(NG):
            forward_group(w - 1, g)
        next_hop()
        for g in range(NG):
            ffn(w - 1, g)
    while todo:
        next_hop()
    forward_group(NW - 1, 0)
    for g in range(half):
        forward_group(NW - 1, g + 1)
        ffn(NW - 1, g)
    down(0)
    for g in range(half, NG):
        if g + 1 < NG:
            forward_group(NW - 1, g + 1)
        ffn(NW - 1, g)
    ahead = 1 if Z > 2 else 0
    if ahead:
        for d in range(ND):
            add_and_pass(0, d, ahead)
    if NS > 1:
        down(1)

    out_copy = pltpu.make_async_copy(out_s, out_hbm, osem)

    def project(n):
        for r in range(Z) if n == 0 else ():
            share(r, pc).wait_recv()
        cols = slice(n * (TOK // 4), (n + 1) * (TOK // 4))
        outt = lax.dot_general(
            wo_s[...], m_s[:, cols], (((0,), (0,)), ((), ())), preferred_element_type=F32
        )
        out_s[cols, :] = outt.T.astype(BF16)
        if n == 3:
            out_copy.start()

    lanes_out = J * 2 * SUB
    lane = lax.broadcasted_iota(jnp.int32, (1, lanes_out), 1)

    def weigh_all():
        token = lax.broadcasted_iota(jnp.int32, (NTOK, lanes_out), 0)
        mine = z * 2 * SUB + lane % (2 * SUB)
        pick = jnp.where(token == mine, 1.0, 0.0).astype(BF16)
        local = slot_s[...] - (z * UNIT).astype(F32)
        local = jnp.where((local >= 0) & (local < UNIT), local, -1.0).astype(BF16)
        place_at = jnp.dot(local, pick, preferred_element_type=F32)
        high = jnp.dot(weight_hi, pick, preferred_element_type=F32)
        low = jnp.dot(weight_lo, pick, preferred_element_type=F32)
        shift = (lane // (2 * SUB) * UNIT).astype(F32)
        target = jnp.where(place_at >= 0, place_at + shift, -1.0)
        row = lax.broadcasted_iota(jnp.int32, (J * UNIT, lanes_out), 0).astype(F32)
        for k in range(E):
            rows = slice(k * J * UNIT, (k + 1) * J * UNIT)
            here = row == target[k : k + 1, :]
            gh_s[rows, :] = jnp.where(here, high[k : k + 1, :], 0.0).astype(BF16)
            gl_s[rows, :] = jnp.where(here, low[k : k + 1, :], 0.0).astype(BF16)

    BR = J * UNIT

    def give_back(k):
        rows = slice(k * BR, (k + 1) * BR)
        return remote(
            fb_s.at[rows, :], rr_s.at[rows, :], rsend.at[k], rrecv.at[k], moved(me, offs[k], E, back=True), t
        )

    side = [functools.partial(project, n) for n in range(4)] + [weigh_all]
    def last(g):
        rows = slice(g * SG * BR, (g + 1) * SG * BR)
        fb_s[rows, :] = jnp.dot(perm_back_s[...], fs_s[g], preferred_element_type=F32).astype(BF16)
        for k in range(g * SG, (g + 1) * SG):
            if k:
                give_back(k).start()

    for s in range(1, Z):
        for g in reversed(range(NS)):
            step = s if g else s + ahead
            if step < Z:
                for d in range(ND):
                    add_and_pass(g, d, step)
            if step == Z - 1:
                last(g)
        if s < Z - 1:
            for _ in range(-(-len(side) // max(1, Z - 1 - s))):
                side.pop(0)()
    while side:
        side.pop(0)()
    rr_s[0:BR, :] = fb_s[0:BR, :]
    for k in range(1, E):
        give_back(k).wait_recv()
    results = rr_s[...].T
    combined = jnp.dot(results, gh_s[...], preferred_element_type=F32) + jnp.dot(
        results, gl_s[...], preferred_element_type=F32
    )
    combined = combined.T.astype(BF16)
    for j in range(J):
        co_s[j] = combined[j * 2 * SUB : (j + 1) * 2 * SUB, :]

    def hand_over(core):
        mine = pl.ds(pl.multiple_of((1 - core) * SUB, SUB), SUB)
        return remote(co_s.at[:, mine, :], mo_s.at[core], zsend, zrecv, me, z * 2 + pc)

    hand_over(c).start()
    mo_s[c] = co_s[:, pl.ds(pl.multiple_of(c * SUB, SUB), SUB), :]
    hand_over(pc).wait_recv()
    for half in range(2):
        for j in range(J):
            moe_ref[:, half * H + j * 128 : half * H + (j + 1) * 128] = mo_s[half, j]

    for k in range(1, E):
        for w in range(NW):
            dispatch(w, k).wait_send()
        hand_on(k).wait_send()
        give_back(k).wait_send()
    for w in range(NW):
        for g in range(NG):
            forward(w, g, c).wait_send()
    for way, half in lanes:
        for hop in range(1, reach[way, half] + 1):
            ring(way, half, hop).wait_send()
    for r in range(Z):
        share(r, c).wait_send()
    for g in range(NS):
        for r in range(Z):
            swap(g, r).wait_send()
        for d in range(ND):
            for s in range(Z - 1):
                pass_on(g, d, s).wait_send()
    hand_over(c).wait_send()
    out_copy.wait()


def settle(a_in, b_in, a_out, b_out, a_s, b_s, sem):
    ins = [pltpu.make_async_copy(a_in, a_s, sem.at[0]), pltpu.make_async_copy(b_in, b_s, sem.at[1])]
    outs = [pltpu.make_async_copy(a_s, a_out, sem.at[2]), pltpu.make_async_copy(b_s, b_out, sem.at[3])]
    for copy in ins:
        copy.start()
    for copy, out in zip(ins, outs):
        copy.wait()
        out.start()
    for out in outs:
        out.wait()


def on_device(
    query, forget, values, out_gate, gap, extra, head_gain, w_out,
    tokens, ff_gain, chosen, chosen_w, w_gate, w_up, w_down,
):
    E, TP = w_gate.shape[0] * lax.axis_size("ep"), lax.axis_size("tp")
    TOK, D = query.shape[0], tokens.shape[1]
    NTOK, FF = tokens.shape[0], w_gate.shape[2]
    SUB = NTOK // TP
    CAP = max(2, SUB * TOPK * 5 // (4 * E))
    Z, KR = TP // 2, TP * CAP
    ROWS, H = E * KR, D // 2
    KG = max(1, E // 4)
    NG = E // KG
    SG = max(1, E // 2)
    NS, UNIT, J = E // SG, 2 * CAP, H // 128
    SR = SG * UNIT
    ND = 4 if H % 512 == 0 else 2
    NW = 2
    cfg = dict(E=E, TP=TP, TOK=TOK, SUB=SUB, CAP=CAP, ND=ND, NW=NW)
    any_spec = pl.BlockSpec(memory_space=pl.ANY)
    hbm = pl.BlockSpec(memory_space=pl.ANY)
    vmem = pl.BlockSpec(memory_space=pltpu.VMEM)
    dma = pltpu.SemaphoreType.DMA
    V = pltpu.VMEM
    hops = Z // 2
    results = pl.pallas_call(
        functools.partial(kernel, cfg),
        out_shape=(
            jax.ShapeDtypeStruct((TOK, w_out.shape[1]), BF16),
            jax.ShapeDtypeStruct((SUB, D), BF16),
        ),
        in_specs=[hbm] * 4 + [vmem] * 3 + [hbm] * 2 + [vmem] * 3 + [hbm] * 3,
        out_specs=(any_spec, vmem),
        scratch_shapes=[
            V((TOK, KEY_DIM), BF16), V((TOK, KEY_DIM), BF16), V((VAL_DIM, TOK), BF16), V((VAL_DIM, TOK), BF16),
            V(w_out.shape, BF16), V((2, NTOK, H), BF16), V((FF, D), BF16), V((FF, D), BF16), V((FF, D), BF16),
            V((PAIR, PAIR), F32), V((TOK // PAIR * 8, KEY_DIM), F32), V((TOK, KEY_DIM), F32),
            V((VAL_DIM, TOK), F32), V((TOK, KEY_DIM), BF16), V((VAL_DIM + 16, KEY_DIM), BF16),
            V((E, VAL_DIM + 16, KEY_DIM), BF16),
            V((NTOK, H), BF16), V((E, NTOK), F32), V((ROWS, NTOK), BF16), V((NW, ROWS, H // NW), BF16),
            V((2, NW, ROWS, H // NW), BF16), V((ROWS, FF), F32), V((ROWS, FF), F32),
            V((ROWS, FF), BF16), V((ROWS, FF), BF16),
            V((2, ND, NS, Z, SR, H // ND), BF16), V((ND, NS, Z, SR, H // ND), BF16),
            V((Z - 1, NS, ND, SR, H // ND), BF16),
            V((Z * SR, Z * SR), BF16), V((J * SR, J * SR), BF16),
            V((TP * VAL_DIM, TOK), BF16), V((TOK, w_out.shape[1]), BF16), V((NS, J * SR, 128), BF16),
            V((E * J * UNIT, 128), BF16), V((E * J * UNIT, 128), BF16),
            V((E * J * UNIT, J * 2 * SUB), BF16), V((E * J * UNIT, J * 2 * SUB), BF16),
            V((J, 2 * SUB, 128), BF16), V((2, J, SUB, 128), BF16),
            dma((10,)), dma, dma((NW, E)), dma((NW, E)), dma((NW, NG)), dma((NW, NG)), dma((E,)), dma((E,)),
            dma((2, 2, hops)), dma((2, 2, hops)), dma((Z,)), dma((Z,)), dma((NS, Z)), dma((NS, Z)),
            dma((Z - 1, NS, ND)), dma((Z - 1, NS, ND)), dma((E,)), dma((E,)), dma, dma,
        ],
        compiler_params=pltpu.CompilerParams(
            collective_id=0, has_side_effects=True, vmem_limit_bytes=64000 * 1024
        ),
    )(
        query, forget, values.T, out_gate.T, gap.reshape(1, -1), extra.T, head_gain.reshape(1, -1), w_out,
        tokens, ff_gain.reshape(1, -1), chosen.T, chosen_w.T, w_gate[0].T, w_up[0].T, w_down[0],
    )
    return pl.pallas_call(
        settle,
        out_shape=tuple(jax.ShapeDtypeStruct(r.shape, r.dtype) for r in results),
        in_specs=[any_spec] * 2,
        out_specs=(any_spec, any_spec),
        scratch_shapes=[V(results[0].shape, BF16), V(results[1].shape, BF16), dma((4,))],
    )(*results)


def solution(mesh):
    placed = (
        P("ep", "tp"), P("ep", "tp"), P("ep", "tp"), P("ep", "tp"), P("tp"), P("ep", "tp"), P("tp"),
        P(None, "tp"), P("ep", None), P(), P("ep", None), P("ep", None),
        P("ep", None, "tp"), P("ep", None, "tp"), P("ep", "tp", None),
    )
    return jax.shard_map(
        on_device,
        mesh=mesh,
        in_specs=placed,
        out_specs=(P("ep", "tp"), P(("ep", "tp"), None)),
        check_vma=False,
    )
```

```python
import functools

import jax
import jax.numpy as jnp
from jax import lax
from jax.experimental import pallas as pl
from jax.experimental.pallas import tpu as pltpu
from jax.sharding import PartitionSpec as P

KEY_DIM = 128
VAL_DIM = 64
BLOCK = 64
PAIR = 128
TOPK = 2
EPS = 1e-06
MESH = pl.DeviceIdType.MESH
F32 = jnp.float32
BF16 = jnp.bfloat16
NT = (((1,), (1,)), ((), ()))


def offsets(experts):
    if experts == 16:
        return [
            (0, 0), (2, 2), (1, 2), (2, 1),
            (3, 2), (2, 3), (0, 1), (3, 0),
            (1, 1), (3, 3), (0, 2), (2, 0),
            (1, 3), (3, 1), (0, 3), (1, 0),
        ]
    return [(0, k) for k in range(experts)]


def moved(me, step, experts, back=False):
    dy, dx = step
    if experts != 16:
        return lax.rem(me + (experts - dx if back else dx), experts)
    y, x = me // 4, lax.rem(me, 4)
    if back:
        dy, dx = (4 - dy) % 4, (4 - dx) % 4
    return lax.rem(y + dy, 4) * 4 + lax.rem(x + dx, 4)


def kernel(
    cfg,
    q_hbm, f_hbm, v_hbm, o_hbm, gap_ref, extra_ref, hgain_ref, wo_hbm,
    x_hbm, fgain_ref, idx_ref, wt_ref, wg_hbm, wu_hbm, wd_hbm,
    out_hbm, moe_ref,
    q_s, f_s, v_s, o_s, wo_s, x_s, wg_s, wu_s, wd_s,
    tri_s, dec_s, pre_s, yw_s, qe_s, cs_s, cr_s,
    n_s, slot_s, g_s, s_s, r_s, ga_s, ua_s, hid_s, hp_s, pp_s, qb_s, rb_s,
    perm_s, perm_back_s, m_s, out_s, fs_s, fb_s, rr_s, gh_s, gl_s, co_s, mo_s,
    lsem, osem, asend, arecv, fsend, frecv, csend, crecv,
    msend, mrecv, dsend, drecv, psend, precv, bsend, brecv, rsend, rrecv, zsend, zrecv,
):
    E, TP, TOK, SUB, CAP = cfg["E"], cfg["TP"], cfg["TOK"], cfg["SUB"], cfg["CAP"]
    Z = TP // 2
    KR = TP * CAP
    KG = max(1, E // 4)
    NG = E // KG
    GR = KG * KR
    UNIT = 2 * CAP
    SG = max(1, E // 2)
    NS = E // SG
    SR = SG * UNIT
    D = x_hbm.shape[1]
    H = D // 2
    ND = cfg["ND"]
    W = H // ND
    NW = cfg["NW"]
    HW = H // NW
    J = H // 128
    NTOK = x_hbm.shape[0]
    offs = offsets(E)
    me = lax.axis_index("ep")
    t = lax.axis_index("tp")
    z, c = t // 2, lax.rem(t, 2)
    pc = 1 - c

    def remote(src, dst, ss, rs, e, tt):
        return pltpu.make_async_remote_copy(
            src_ref=src, dst_ref=dst, send_sem=ss, recv_sem=rs, device_id=(e, tt), device_id_type=MESH
        )

    loads = [
        (f_hbm, f_s), (q_hbm, q_s), (v_hbm, v_s), (x_hbm.at[:, 0:H], x_s.at[0]), (x_hbm.at[:, H:D], x_s.at[1]),
        (o_hbm, o_s),
        (wg_hbm, wg_s), (wu_hbm, wu_s), (wd_hbm, wd_s), (wo_hbm, wo_s),
    ]
    loads = [pltpu.make_async_copy(a, b, lsem.at[i]) for i, (a, b) in enumerate(loads)]
    for load in loads:
        load.start()
    barrier = pltpu.get_barrier_semaphore()
    for k in range(1, E):
        pl.semaphore_signal(barrier, inc=1, device_id=(moved(me, offs[k], E), t), device_id_type=MESH)
    for j in (z * 2 + pc, lax.rem(z + 1, Z) * 2 + c, lax.rem(z + Z - 1, Z) * 2 + c):
        pl.semaphore_signal(barrier, inc=1, device_id=(me, j), device_id_type=MESH)

    i0, i1 = idx_ref[0:1, :], idx_ref[1:2, :]
    row_e = lax.broadcasted_iota(jnp.int32, (E, NTOK), 0)
    expert_of = jnp.zeros((E, NTOK), jnp.int32)
    for k in range(E):
        expert_of = jnp.where(row_e == k, moved(me, offs[k], E), expert_of)
    first, second = expert_of == i0, expert_of == i1
    chosen = jnp.where(first | second, 1.0, 0.0)
    ra = lax.broadcasted_iota(jnp.int32, (NTOK, NTOK), 0)
    rb = lax.broadcasted_iota(jnp.int32, (NTOK, NTOK), 1)
    before = jnp.where((ra // SUB == rb // SUB) & (ra < rb), 1.0, 0.0).astype(BF16)
    place = jnp.dot(chosen.astype(BF16), before, preferred_element_type=F32)
    block_of = (lax.broadcasted_iota(jnp.int32, (E, NTOK), 1) // SUB).astype(F32)
    slot_s[...] = jnp.where(chosen > 0, CAP * block_of + place, -1.0)
    weight = jnp.where(first, wt_ref[0:1, :], 0.0) + jnp.where(second, wt_ref[1:2, :], 0.0)
    weight_hi = weight.astype(BF16)
    weight_lo = (weight - weight_hi.astype(F32)).astype(BF16)

    place_row = lax.broadcasted_iota(jnp.int32, (KR, NTOK), 0).astype(F32)

    def fill_group(g):
        for k in range(g * KG, (g + 1) * KG):
            rows = slice(k * KR, (k + 1) * KR)
            g_s[rows, :] = jnp.where(place_row == slot_s[k : k + 1, :], 1.0, 0.0).astype(BF16)
        rows = slice(g * GR, (g + 1) * GR)
        pick = g_s[rows, :]
        for n in range(0, H, min(HW, 256)):
            at = n % HW
            s_s[n // HW, rows, at : at + min(HW, 256)] = jnp.dot(
                pick, n_s[:, n : n + min(HW, 256)], preferred_element_type=F32
            ).astype(BF16)

    def dispatch(w, k):
        rows = slice(k * KR, (k + 1) * KR)
        return remote(
            s_s.at[w, rows, :], r_s.at[c, w, rows, :], asend.at[w, k], arecv.at[w, k],
            moved(me, offs[k], E), t,
        )

    def forward(w, g, core):
        rows = slice(g * GR, (g + 1) * GR)
        return remote(
            r_s.at[core, w, rows, :], r_s.at[core, w, rows, :], fsend.at[w, g], frecv.at[w, g], me, z * 2 + pc
        )

    ta = lax.broadcasted_iota(jnp.int32, (PAIR, PAIR), 0)
    tb = lax.broadcasted_iota(jnp.int32, (PAIR, PAIR), 1)
    tri = (ta // BLOCK == tb // BLOCK) & (ta >= tb)
    tri_s[...] = jnp.where(tri, 1.0, 0.0)
    gap = gap_ref[...]
    for load in loads[0:3]:
        load.wait()
    U1 = min(4, TOK // PAIR)

    def local_pairs(i, carry):
        state, decay = carry
        trif = tri_s[...]
        trib = trif.astype(BF16)
        in_first = lax.broadcasted_iota(jnp.int32, (PAIR, PAIR), 0) < BLOCK
        left = lax.broadcasted_iota(jnp.int32, (BLOCK, PAIR), 1) < BLOCK
        later = lax.broadcasted_iota(jnp.int32, (PAIR, PAIR), 1)
        earlier = lax.broadcasted_iota(jnp.int32, (PAIR, PAIR), 0)
        maskt = (later // BLOCK == earlier // BLOCK) & (earlier <= later)
        at = [pl.multiple_of((i * U1 + u) * PAIR, PAIR) for u in range(U1)]
        keys, cums = [], []
        for u in range(U1):
            gate = f_s[pl.ds(at[u], PAIR), :].astype(F32)
            key = gap * (1.0 / (1.0 + jnp.exp(gate)))
            logf = jnp.log(1.0 - key)
            hi = logf.astype(BF16)
            lo = (logf - hi.astype(F32)).astype(BF16)
            cum = jnp.dot(trib, hi, preferred_element_type=F32) + jnp.dot(
                trib, lo, preferred_element_type=F32
            )
            extra = jnp.sum(trif * extra_ref[:, pl.ds(at[u], PAIR)], axis=-1, keepdims=True)
            keys.append(key)
            cums.append(cum + extra)
        work = []
        for u in range(U1):
            key, cum = keys[u], cums[u]
            mid0, mid1 = cum[31:32, :], cum[95:96, :]
            end0, end1 = cum[63:64, :], cum[127:128, :]
            away = cum - jnp.where(in_first, mid0, mid1)
            query = q_s[pl.ds(at[u], PAIR), :].astype(F32)
            query = query * (1.0 / (1.0 + jnp.exp(-query)))
            qs = query * jnp.exp(away)
            ks = key * jnp.exp(-away)
            qe = qs * jnp.where(in_first, jnp.exp(mid0), jnp.exp(mid1))
            ke = ks * jnp.where(in_first, jnp.exp(end0 - mid0), jnp.exp(end1 - mid1))
            qe_s[pl.ds(at[u], PAIR), :] = qe.astype(BF16)
            work.append((qs.astype(BF16), ks.astype(BF16), ke.astype(BF16), jnp.exp(end0), jnp.exp(end1)))
        scores = [lax.dot_general(w[1], w[0], NT, preferred_element_type=F32) for w in work]
        updates = []
        for u in range(U1):
            vt = v_s[:, pl.ds(at[u], PAIR)]
            both = jnp.where(maskt, scores[u], 0.0).astype(BF16)
            yw_s[:, pl.ds(at[u], PAIR)] = jnp.dot(vt, both, preferred_element_type=F32)
            zero = jnp.zeros_like(vt)
            split = jnp.concatenate([jnp.where(left, vt, zero), jnp.where(left, zero, vt)], axis=0)
            updates.append(jnp.dot(split, work[u][2], preferred_element_type=F32))
        for u in range(U1):
            d0, d1 = work[u][3], work[u][4]
            middle = d0 * state + updates[u][0:BLOCK, :]
            pre_s[pl.ds(at[u], BLOCK), :] = state
            pre_s[pl.ds(pl.multiple_of(at[u] + BLOCK, BLOCK), BLOCK), :] = middle
            half = decay * d0
            dec_s[pl.ds(pl.multiple_of((i * U1 + u) * 8, 8), 8), :] = jnp.concatenate(
                [decay, half, jnp.zeros((6, KEY_DIM), F32)], axis=0
            )
            state = d1 * middle + updates[u][BLOCK:PAIR, :]
            decay = half * d1
        return state, decay

    state, decay = lax.fori_loop(
        0, TOK // (PAIR * U1), local_pairs,
        (jnp.zeros((VAL_DIM, KEY_DIM), F32), jnp.ones((1, KEY_DIM), F32)),
    )
    decay_hi = decay.astype(BF16).astype(F32)
    row16 = lax.broadcasted_iota(jnp.int32, (16, KEY_DIM), 0)
    tail = jnp.where(row16 == 0, decay_hi, jnp.where(row16 == 1, decay - decay_hi, 0.0))
    cs_s[0:VAL_DIM, :] = state.astype(BF16)
    cs_s[VAL_DIM : VAL_DIM + 16, :] = tail.astype(BF16)
    cr_s[me] = jnp.zeros((VAL_DIM + 16, KEY_DIM), BF16)

    def hand_on(k):
        return remote(cs_s, cr_s.at[me], csend.at[k], crecv.at[me], moved(me, offs[k], E), t)

    def handed(k):
        source = moved(me, offs[k], E, back=True)
        return remote(cs_s, cr_s.at[source], csend.at[k], crecv.at[source], source, t)

    pl.semaphore_wait(barrier, E - 1 + 3)
    for k in range(1, E):
        pl.when(moved(me, offs[k], E) > me)(hand_on(k).start)

    loads[3].wait()
    loads[4].wait()
    gain_half = fgain_ref[:, pl.ds(pl.multiple_of(c * H, 128), H)]

    def norm_rows(i, carry):
        rows = pl.ds(pl.multiple_of(i * 64, 64), 64)
        a, b = x_s[0, rows, :].astype(F32), x_s[1, rows, :].astype(F32)
        total = jnp.sum(a * a + b * b, axis=-1, keepdims=True)
        factor = lax.rsqrt(total / D + EPS)
        n_s[rows, :] = (x_s[c, rows, :].astype(F32) * factor * gain_half).astype(BF16)
        return carry

    lax.fori_loop(0, NTOK // 64, norm_rows, 0)

    for g in range(NG):
        fill_group(g)
    r_s[c, :, 0:KR, :] = s_s[:, 0:KR, :]
    for k in range(1, E):
        pl.when(moved(me, offs[k], E, back=True) < me)(handed(k).wait_recv)
    for k in range(1, E):
        dispatch(0, k).start()

    start = jnp.zeros((VAL_DIM, KEY_DIM), F32)
    for j in range(E - 1):
        ends = cr_s[j, VAL_DIM : VAL_DIM + 16, :].astype(F32)
        after = (ends[0:1, :] + ends[1:2, :]) * start + cr_s[j, 0:VAL_DIM, :].astype(F32)
        start = jnp.where(j < me, after, start)
    ga = lax.broadcasted_iota(jnp.int32, (VAL_DIM, VAL_DIM), 0)
    gb = lax.broadcasted_iota(jnp.int32, (VAL_DIM, VAL_DIM), 1)
    head_gain = jnp.sum(jnp.where(ga == gb, hgain_ref[...], 0.0), axis=-1, keepdims=True)
    own_rows = pl.multiple_of(t * VAL_DIM, VAL_DIM)

    loads[5].wait()

    def finish_pairs(i, carry):
        left = lax.broadcasted_iota(jnp.int32, (BLOCK, PAIR), 1) < BLOCK
        at = [pl.multiple_of((i * U1 + u) * PAIR, PAIR) for u in range(U1)]
        across = []
        for u in range(U1):
            d = dec_s[pl.ds(pl.multiple_of((i * U1 + u) * 8, 8), 8), :]
            s0 = pre_s[pl.ds(at[u], BLOCK), :] + d[0:1, :] * start
            s1 = pre_s[pl.ds(pl.multiple_of(at[u] + BLOCK, BLOCK), BLOCK), :] + d[1:2, :] * start
            states = jnp.concatenate([s0, s1], axis=0).astype(BF16)
            across.append(
                lax.dot_general(states, qe_s[pl.ds(at[u], PAIR), :], NT, preferred_element_type=F32)
            )
        for u in range(U1):
            cols = pl.ds(at[u], PAIR)
            y = yw_s[:, cols] + jnp.where(left, across[u][0:BLOCK, :], across[u][BLOCK:PAIR, :])
            factor = lax.rsqrt(jnp.mean(y * y, axis=0, keepdims=True) + EPS)
            gate = o_s[:, cols].astype(F32)
            gate = gate * (1.0 / (1.0 + jnp.exp(-gate)))
            m_s[pl.ds(own_rows, VAL_DIM), cols] = (y * factor * head_gain * gate).astype(BF16)
        return carry

    lax.fori_loop(0, TOK // (PAIR * U1), finish_pairs, 0)

    VH = VAL_DIM // 2
    reach = {(1, 0): Z // 2, (1, 1): Z - 1 - Z // 2, (-1, 0): Z - 1 - Z // 2, (-1, 1): Z // 2}

    def head_at(zz, core):
        return pl.multiple_of((lax.rem(zz + 2 * Z, Z) * 2 + core) * VAL_DIM, VAL_DIM)

    def ring(way, half, hop):
        rows = pl.ds(pl.multiple_of(head_at(z - way * (hop - 1), c) + half * VH, VH), VH)
        w = 0 if way == 1 else 1
        return remote(
            m_s.at[rows, :], m_s.at[rows, :], msend.at[w, half, hop - 1], mrecv.at[w, half, hop - 1],
            me, lax.rem(z + way + Z, Z) * 2 + c,
        )

    def ringed(way, half, hop):
        rows = pl.ds(pl.multiple_of(head_at(z - way * hop, c) + half * VH, VH), VH)
        w = 0 if way == 1 else 1
        return remote(
            m_s.at[rows, :], m_s.at[rows, :], msend.at[w, half, hop - 1], mrecv.at[w, half, hop - 1],
            me, lax.rem(z + way + Z, Z) * 2 + c,
        )

    def share(r, core):
        rows = pl.ds(head_at(z - r, core), VAL_DIM)
        return remote(m_s.at[rows, :], m_s.at[rows, :], dsend.at[r], drecv.at[r], me, z * 2 + pc)

    lanes = [(1, 0), (-1, 1), (1, 1), (-1, 0)]

    def relay(hop):
        for way, half in lanes:
            if hop <= reach[way, half]:
                ringed(way, half, hop).wait_recv()
                if hop + 1 <= reach[way, half]:
                    ring(way, half, hop + 1).start()
        if hop == Z - hop:
            share(hop, c).start()
        elif hop < Z - hop:
            share(hop, c).start()
            share(Z - hop, c).start()

    for way, half in lanes:
        if reach[way, half] >= 1:
            ring(way, half, 1).start()
    share(0, c).start()

    def swapper(ref, outer, inner):
        size = outer * inner * UNIT
        row = lax.broadcasted_iota(jnp.int32, (size, 1), 0)
        source = (row // UNIT % inner * outer + row // (inner * UNIT)) * UNIT + row % UNIT
        ref[...] = jnp.where(lax.broadcasted_iota(jnp.int32, (size, size), 1) == source, 1.0, 0.0).astype(BF16)

    swapper(perm_s, Z, SG)
    swapper(perm_back_s, SG, J)

    def forward_group(w, g):
        for k in range(g * KG, (g + 1) * KG):
            if k:
                dispatch(w, k).wait_recv()
        forward(w, g, c).start()

    def ffn(w, g):
        rows = slice(g * GR, (g + 1) * GR)
        forward(w, g, pc).wait_recv()
        a, b = r_s[0, w, rows, :], r_s[1, w, rows, :]
        ca, cb = slice(w * HW, (w + 1) * HW), slice(H + w * HW, H + (w + 1) * HW)

        def product(weight):
            return lax.dot_general(a, weight[:, ca], NT, preferred_element_type=F32) + lax.dot_general(
                b, weight[:, cb], NT, preferred_element_type=F32
            )

        gate, up = product(wg_s), product(wu_s)
        if w:
            gate, up = gate + ga_s[rows, :], up + ua_s[rows, :]
        if w < NW - 1:
            ga_s[rows, :] = gate
            ua_s[rows, :] = up
        else:
            hid_s[rows, :] = (gate * (1.0 / (1.0 + jnp.exp(-gate))) * up).astype(BF16)

    def relative(r):
        return lax.rem(z + r + 2 * Z, Z)

    def swap(g, r):
        part = relative(r)
        return remote(
            pp_s.at[pc, :, g, part], qb_s.at[:, g, part], psend.at[g, r % Z], precv.at[g, r % Z],
            me, z * 2 + pc,
        )

    def way_of(d):
        return 1 - 2 * (d % 2)

    def pass_on(g, d, s):
        way = way_of(d)
        part = relative(-way * (1 + s))
        return remote(
            pp_s.at[c, d, g, part], rb_s.at[s, g, d], bsend.at[s, g, d], brecv.at[s, g, d],
            me, relative(way) * 2 + c,
        )

    swapped = set()

    def add_and_pass(g, d, s):
        r = -way_of(d) * (1 + s)
        part = relative(r)
        if (g, r % Z) not in swapped:
            swapped.add((g, r % Z))
            swap(g, r).wait_recv()
        total = pp_s[c, d, g, part].astype(F32) + qb_s[d, g, part].astype(F32)
        if s:
            pass_on(g, d, s - 1).wait_recv()
            total = total + rb_s[s - 1, g, d].astype(F32)
        if s < Z - 1:
            pp_s[c, d, g, part] = total.astype(BF16)
            pass_on(g, d, s).start()
        else:
            for n in range(W // 128):
                at = (d * (W // 128) + n) * SR
                fs_s[g, at : at + SR, :] = total[:, n * 128 : n * 128 + 128].astype(BF16)

    def down(g, between=None):
        rows = slice(g * Z * SR, (g + 1) * Z * SR)
        hp_s[rows, :] = jnp.dot(
            perm_s[...], hid_s[rows, :], preferred_element_type=F32
        ).astype(BF16)
        turns = [r for n in range(1, Z // 2) for r in (-n, n)] + [Z // 2, 0]
        for n in range(0, Z, 2):
            pair = turns[n : n + 2]
            hid = jnp.concatenate(
                [
                    hp_s[pl.ds(pl.multiple_of((g * Z + relative(r)) * SR, 16), SR), :]
                    for r in pair
                ],
                axis=0,
            )
            for half in range(2):
                for d in range(ND):
                    cols = slice(half * H + d * W, half * H + (d + 1) * W)
                    y = jnp.dot(hid, wd_s[:, cols], preferred_element_type=F32).astype(BF16)
                    for i, r in enumerate(pair):
                        pp_s[half, d, g, relative(r)] = y[i * SR : (i + 1) * SR, :]
            for r in pair:
                swap(g, r).start()
            if between and n == 2:
                between()
            if n == min(2, Z - 2):
                for d in range(ND):
                    add_and_pass(g, d, 0)

    hops = max(reach.values())
    for load in loads[6:]:
        load.wait()
    half = NG // 2
    todo = list(range(1, hops + 1))

    def next_hop():
        if todo:
            relay(todo.pop(0))

    next_hop()
    for w in range(1, NW):
        for k in range(1, E):
            dispatch(w, k).start()
        for g in range(NG):
            forward_group(w - 1, g)
        next_hop()
        for g in range(NG):
            ffn(w - 1, g)
    while todo:
        next_hop()
    forward_group(NW - 1, 0)
    for g in range(half):
        forward_group(NW - 1, g + 1)
        ffn(NW - 1, g)
    down(0)
    for g in range(half, NG):
        if g + 1 < NG:
            forward_group(NW - 1, g + 1)
        ffn(NW - 1, g)
    ahead = 1 if Z > 2 else 0
    if ahead:
        for d in range(ND):
            add_and_pass(0, d, ahead)
    if NS > 1:
        down(1)

    out_copy = pltpu.make_async_copy(out_s, out_hbm, osem)

    def project(n):
        for r in range(Z) if n == 0 else ():
            share(r, pc).wait_recv()
        cols = slice(n * (TOK // 4), (n + 1) * (TOK // 4))
        outt = lax.dot_general(
            wo_s[...], m_s[:, cols], (((0,), (0,)), ((), ())), preferred_element_type=F32
        )
        out_s[cols, :] = outt.T.astype(BF16)
        if n == 3:
            out_copy.start()

    lanes_out = J * 2 * SUB
    lane = lax.broadcasted_iota(jnp.int32, (1, lanes_out), 1)

    def weigh_all():
        token = lax.broadcasted_iota(jnp.int32, (NTOK, lanes_out), 0)
        mine = z * 2 * SUB + lane % (2 * SUB)
        pick = jnp.where(token == mine, 1.0, 0.0).astype(BF16)
        local = slot_s[...] - (z * UNIT).astype(F32)
        local = jnp.where((local >= 0) & (local < UNIT), local, -1.0).astype(BF16)
        place_at = jnp.dot(local, pick, preferred_element_type=F32)
        high = jnp.dot(weight_hi, pick, preferred_element_type=F32)
        low = jnp.dot(weight_lo, pick, preferred_element_type=F32)
        shift = (lane // (2 * SUB) * UNIT).astype(F32)
        target = jnp.where(place_at >= 0, place_at + shift, -1.0)
        row = lax.broadcasted_iota(jnp.int32, (J * UNIT, lanes_out), 0).astype(F32)
        for k in range(E):
            rows = slice(k * J * UNIT, (k + 1) * J * UNIT)
            here = row == target[k : k + 1, :]
            gh_s[rows, :] = jnp.where(here, high[k : k + 1, :], 0.0).astype(BF16)
            gl_s[rows, :] = jnp.where(here, low[k : k + 1, :], 0.0).astype(BF16)

    BR = J * UNIT

    def give_back(k):
        rows = slice(k * BR, (k + 1) * BR)
        return remote(
            fb_s.at[rows, :], rr_s.at[rows, :], rsend.at[k], rrecv.at[k], moved(me, offs[k], E, back=True), t
        )

    side = [functools.partial(project, n) for n in range(4)] + [weigh_all]
    def last(g):
        rows = slice(g * SG * BR, (g + 1) * SG * BR)
        fb_s[rows, :] = jnp.dot(perm_back_s[...], fs_s[g], preferred_element_type=F32).astype(BF16)
        for k in range(g * SG, (g + 1) * SG):
            if k:
                give_back(k).start()

    for s in range(1, Z):
        for g in reversed(range(NS)):
            step = s if g else s + ahead
            if step < Z:
                for d in range(ND):
                    add_and_pass(g, d, step)
            if step == Z - 1:
                last(g)
        if s < Z - 1:
            for _ in range(-(-len(side) // max(1, Z - 1 - s))):
                side.pop(0)()
    while side:
        side.pop(0)()
    rr_s[0:BR, :] = fb_s[0:BR, :]
    for k in range(1, E):
        give_back(k).wait_recv()
    results = rr_s[...].T
    combined = jnp.dot(results, gh_s[...], preferred_element_type=F32) + jnp.dot(
        results, gl_s[...], preferred_element_type=F32
    )
    combined = combined.T.astype(BF16)
    for j in range(J):
        co_s[j] = combined[j * 2 * SUB : (j + 1) * 2 * SUB, :]

    def hand_over(core):
        mine = pl.ds(pl.multiple_of((1 - core) * SUB, SUB), SUB)
        return remote(co_s.at[:, mine, :], mo_s.at[core], zsend, zrecv, me, z * 2 + pc)

    hand_over(c).start()
    mo_s[c] = co_s[:, pl.ds(pl.multiple_of(c * SUB, SUB), SUB), :]
    hand_over(pc).wait_recv()
    for half in range(2):
        for j in range(J):
            moe_ref[:, half * H + j * 128 : half * H + (j + 1) * 128] = mo_s[half, j]

    for k in range(1, E):
        for w in range(NW):
            dispatch(w, k).wait_send()
        pl.when(moved(me, offs[k], E) > me)(hand_on(k).wait_send)
        give_back(k).wait_send()
    for w in range(NW):
        for g in range(NG):
            forward(w, g, c).wait_send()
    for way, half in lanes:
        for hop in range(1, reach[way, half] + 1):
            ring(way, half, hop).wait_send()
    for r in range(Z):
        share(r, c).wait_send()
    for g in range(NS):
        for r in range(Z):
            swap(g, r).wait_send()
        for d in range(ND):
            for s in range(Z - 1):
                pass_on(g, d, s).wait_send()
    hand_over(c).wait_send()
    out_copy.wait()


def settle(a_in, b_in, a_out, b_out, a_s, b_s, sem):
    ins = [pltpu.make_async_copy(a_in, a_s, sem.at[0]), pltpu.make_async_copy(b_in, b_s, sem.at[1])]
    outs = [pltpu.make_async_copy(a_s, a_out, sem.at[2]), pltpu.make_async_copy(b_s, b_out, sem.at[3])]
    for copy in ins:
        copy.start()
    for copy, out in zip(ins, outs):
        copy.wait()
        out.start()
    for out in outs:
        out.wait()


def on_device(
    query, forget, values, out_gate, gap, extra, head_gain, w_out,
    tokens, ff_gain, chosen, chosen_w, w_gate, w_up, w_down,
):
    E, TP = w_gate.shape[0] * lax.axis_size("ep"), lax.axis_size("tp")
    TOK, D = query.shape[0], tokens.shape[1]
    NTOK, FF = tokens.shape[0], w_gate.shape[2]
    SUB = NTOK // TP
    CAP = max(2, SUB * TOPK * 5 // (4 * E))
    Z, KR = TP // 2, TP * CAP
    ROWS, H = E * KR, D // 2
    KG = max(1, E // 4)
    NG = E // KG
    SG = max(1, E // 2)
    NS, UNIT, J = E // SG, 2 * CAP, H // 128
    SR = SG * UNIT
    ND = 4 if H % 512 == 0 else 2
    NW = 2
    cfg = dict(E=E, TP=TP, TOK=TOK, SUB=SUB, CAP=CAP, ND=ND, NW=NW)
    any_spec = pl.BlockSpec(memory_space=pl.ANY)
    hbm = pl.BlockSpec(memory_space=pl.ANY)
    vmem = pl.BlockSpec(memory_space=pltpu.VMEM)
    dma = pltpu.SemaphoreType.DMA
    V = pltpu.VMEM
    hops = Z // 2
    results = pl.pallas_call(
        functools.partial(kernel, cfg),
        out_shape=(
            jax.ShapeDtypeStruct((TOK, w_out.shape[1]), BF16),
            jax.ShapeDtypeStruct((SUB, D), BF16),
        ),
        in_specs=[hbm] * 4 + [vmem] * 3 + [hbm] * 2 + [vmem] * 3 + [hbm] * 3,
        out_specs=(any_spec, vmem),
        scratch_shapes=[
            V((TOK, KEY_DIM), BF16), V((TOK, KEY_DIM), BF16), V((VAL_DIM, TOK), BF16), V((VAL_DIM, TOK), BF16),
            V(w_out.shape, BF16), V((2, NTOK, H), BF16), V((FF, D), BF16), V((FF, D), BF16), V((FF, D), BF16),
            V((PAIR, PAIR), F32), V((TOK // PAIR * 8, KEY_DIM), F32), V((TOK, KEY_DIM), F32),
            V((VAL_DIM, TOK), F32), V((TOK, KEY_DIM), BF16), V((VAL_DIM + 16, KEY_DIM), BF16),
            V((E, VAL_DIM + 16, KEY_DIM), BF16),
            V((NTOK, H), BF16), V((E, NTOK), F32), V((ROWS, NTOK), BF16), V((NW, ROWS, H // NW), BF16),
            V((2, NW, ROWS, H // NW), BF16), V((ROWS, FF), F32), V((ROWS, FF), F32),
            V((ROWS, FF), BF16), V((ROWS, FF), BF16),
            V((2, ND, NS, Z, SR, H // ND), BF16), V((ND, NS, Z, SR, H // ND), BF16),
            V((Z - 1, NS, ND, SR, H // ND), BF16),
            V((Z * SR, Z * SR), BF16), V((J * SR, J * SR), BF16),
            V((TP * VAL_DIM, TOK), BF16), V((TOK, w_out.shape[1]), BF16), V((NS, J * SR, 128), BF16),
            V((E * J * UNIT, 128), BF16), V((E * J * UNIT, 128), BF16),
            V((E * J * UNIT, J * 2 * SUB), BF16), V((E * J * UNIT, J * 2 * SUB), BF16),
            V((J, 2 * SUB, 128), BF16), V((2, J, SUB, 128), BF16),
            dma((10,)), dma, dma((NW, E)), dma((NW, E)), dma((NW, NG)), dma((NW, NG)), dma((E,)), dma((E,)),
            dma((2, 2, hops)), dma((2, 2, hops)), dma((Z,)), dma((Z,)), dma((NS, Z)), dma((NS, Z)),
            dma((Z - 1, NS, ND)), dma((Z - 1, NS, ND)), dma((E,)), dma((E,)), dma, dma,
        ],
        compiler_params=pltpu.CompilerParams(
            collective_id=0, has_side_effects=True, vmem_limit_bytes=64000 * 1024
        ),
    )(
        query, forget, values.T, out_gate.T, gap.reshape(1, -1), extra.T, head_gain.reshape(1, -1), w_out,
        tokens, ff_gain.reshape(1, -1), chosen.T, chosen_w.T, w_gate[0].T, w_up[0].T, w_down[0],
    )
    return pl.pallas_call(
        settle,
        out_shape=tuple(jax.ShapeDtypeStruct(r.shape, r.dtype) for r in results),
        in_specs=[any_spec] * 2,
        out_specs=(any_spec, any_spec),
        scratch_shapes=[V(results[0].shape, BF16), V(results[1].shape, BF16), dma((4,))],
    )(*results)


def solution(mesh):
    placed = (
        P("ep", "tp"), P("ep", "tp"), P("ep", "tp"), P("ep", "tp"), P("tp"), P("ep", "tp"), P("tp"),
        P(None, "tp"), P("ep", None), P(), P("ep", None), P("ep", None),
        P("ep", None, "tp"), P("ep", None, "tp"), P("ep", "tp", None),
    )
    return jax.shard_map(
        on_device,
        mesh=mesh,
        in_specs=placed,
        out_specs=(P("ep", "tp"), P(("ep", "tp"), None)),
        check_vma=False,
    )
```
